512 devices in a mesh: sp: 64 (over z, y), tp: 8 (over x, core).
Axes of the slice: x: 4, y: 8, z: 8, core: 2. Of those that a mesh axis runs over, the one named last changes fastest.
Arguments:
- tokens: bfloat16 [18432, 4096], P('sp', 'tp'), may hold values from -6 to 6
- doc_ids: int32 [18432], P('sp'), may hold values from 0 to 15, never falling along the last dimension, each value on 1 to 9216 neighbouring positions
- norm_gain: float32 [2, 4096], replicated, may hold values from 0.1 to 1.9
- in_proj: bfloat16 [2, 4096, 4096], P(None, 'sp', 'tp'), may hold values from -0.09375 to 0.09375
- mix_proj: bfloat16 [2, 1024, 4096], P(None, 'sp', 'tp'), may hold values from -0.1875 to 0.1875
- out_scale: float32 [2, 4096], replicated, may hold values from 0.1 to 1.9
Outputs:
- mixed_out: bfloat16 [18432, 4096], P('sp', 'tp')
The draws below stay inside these ranges and needn't reach their ends.
Inputs may be any that keep to these rules, and one draw needn't show every extreme that they name: `doc_ids`: document numbers never fall along the sequence, run from 0 to 15, and each document holds at most 9216 positions.
All inputs are finite; a program needn't handle non-finite values.
Results may differ from the reference program's by a relative error of at most 0.0085.
Values may be sent and summed in bfloat16 or wider, within the bound.
A program may use at most 128 MiB of HBM per device.

```python
import math
import jax
import jax.numpy as jnp
import numpy as np
from jax import lax

D = 4096
GROUP = 1024
WIN = 16
LAYERS = 2
TOKENS = 18432
DOCS = 16


def block_levels(key, extent, shards, low, largest):
    gain, own = 1.0, jax.random.fold_in(key, 6)
    for dim, shards_of in shards:
        heights = jnp.exp(jax.random.uniform(jax.random.fold_in(own, dim), (shards_of,), jnp.float32, low / len(shards), largest / len(shards)))
        gain = gain * jnp.repeat(heights, extent[dim] // shards_of).reshape([-1 if axis == dim else 1 for axis in range(len(extent))])
    return gain


def length_profile(count, total, most, skew):
    weights = [(1 << 20) // math.isqrt(standing ** skew) + 1 for standing in range(2, count + 1)]
    rest, counts = total - most - (count - 1), [1] * (count - 1)
    while rest > 0:
        free = [i for i in range(count - 1) if counts[i] < most]
        whole, budget = sum([weights[i] for i in free]), rest
        for i in free:
            extra = min(most - counts[i], max(1, budget * weights[i] // whole), rest)
            counts[i] = counts[i] + extra
            rest = rest - extra
    return np.array([most] + counts)


def uneven(stream_key, amount, total, most, slope):
    if amount == 2:
        one = jax.random.randint(stream_key, (), max(1, total - most), min(most, total - 1) + 1)
        return jnp.stack([one, total - one])
    tallies = jnp.asarray(length_profile(amount, total, most, slope), jnp.int32)
    couples = (amount - 1) // 2
    source_of, taker = tallies[1:1 + 2 * couples:2], tallies[2:2 + 2 * couples:2]
    margin = jnp.minimum(source_of - 1, most - taker)
    moved = jax.random.randint(jax.random.fold_in(stream_key, 1), (couples,), 0, 1 << 20) % (margin + 1)
    tallies = tallies.at[1:1 + 2 * couples:2].set(source_of - moved).at[2:2 + 2 * couples:2].set(taker + moved)
    return tallies[jax.random.permutation(jax.random.fold_in(stream_key, 2), amount)]


def scatter_about(rng, dims, spread, limit, shards=(), kind=jnp.bfloat16):
    values = spread * jax.random.normal(rng, dims, jnp.float32)
    if shards:
        values = values * block_levels(rng, dims, shards, -0.22, 0.18)
    return jnp.clip(values, -limit, limit).astype(kind)


def setup_inputs(seed: int = 0) -> dict:
    splits = jax.random.split(jax.random.key(seed), 7)
    tokens = scatter_about(splits[0], (TOKENS, D), 1.0, 6.0, ((0, 64), (1, 8)))
    doc_ids = jnp.searchsorted(jnp.cumsum(uneven(splits[1], DOCS, TOKENS, TOKENS // 2, 1)), jnp.arange(TOKENS), side="right").astype(jnp.int32)
    norm_gain = jnp.clip(1.0 + 0.18 * jax.random.normal(splits[2], (LAYERS, D), jnp.float32), 0.1, 1.9)
    in_proj = scatter_about(splits[3], (LAYERS, D, D), D ** -0.5, 0.09375, ((1, 64), (2, 8)))
    mix_proj = scatter_about(splits[4], (LAYERS, GROUP, D), GROUP ** -0.5, 0.1875, ((1, 64), (2, 8)))
    out_scale = jnp.clip(1.0 + 0.18 * jax.random.normal(splits[5], (LAYERS, D), jnp.float32), 0.1, 1.9)
    return {"tokens": tokens, "doc_ids": doc_ids, "norm_gain": norm_gain, "in_proj": in_proj, "mix_proj": mix_proj, "out_scale": out_scale}


epsilon = 1e-06

def pool_all(proj_f32, doc_ids, windows):
    padded = jnp.concatenate([jnp.zeros((WIN - 1, D), jnp.float32), proj_f32], axis=0)
    padded_docs = jnp.concatenate([jnp.full((WIN - 1,), -1, jnp.int32), doc_ids.astype(jnp.int32)], axis=0)
    window_sum = jnp.zeros_like(proj_f32)
    window_count = jnp.zeros_like(proj_f32)
    for offset in range(WIN):
        begin = WIN - 1 - offset
        shifted = padded[begin:begin + TOKENS]
        same_doc = padded_docs[begin:begin + TOKENS] == doc_ids
        taken = same_doc[:, None] & (offset < windows)[None, :]
        window_sum = window_sum + jnp.where(taken, shifted, jnp.float32(0.0))
        window_count = window_count + taken.astype(jnp.float32)
    return (window_sum / window_count - proj_f32).astype(jnp.bfloat16)

def reference(tokens, doc_ids, norm_gain, in_proj, mix_proj, out_scale):
    block_width = D // 8
    channels = jnp.arange(D, dtype=jnp.int32)
    windows = jnp.left_shift(jnp.int32(2), channels // block_width % 4)
    current = tokens
    for depth_idx in range(LAYERS):
        values = current.astype(jnp.float32)
        scaled = values * lax.rsqrt(lax.optimization_barrier(jnp.mean(values * values, axis=-1, keepdims=True)) + epsilon)
        normed = (scaled * norm_gain[depth_idx][None, :]).astype(jnp.bfloat16)
        projected = jnp.dot(normed, in_proj[depth_idx], preferred_element_type=jnp.float32).astype(jnp.bfloat16)
        pooled = pool_all(projected.astype(jnp.float32), doc_ids, windows)
        blocks_out = [None] * 8
        for group_idx in range(4):
            first = group_idx * block_width
            second = (group_idx + 4) * block_width
            inputs = jnp.concatenate([pooled[:, first:first + block_width], pooled[:, second:second + block_width]], axis=1)
            weights = jnp.concatenate([mix_proj[depth_idx][:, first:first + block_width], mix_proj[depth_idx][:, second:second + block_width]], axis=1)
            result = jnp.dot(inputs, weights, preferred_element_type=jnp.float32)
            blocks_out[group_idx] = result[:, :block_width]
            blocks_out[group_idx + 4] = result[:, block_width:]
        grouped = jnp.concatenate(blocks_out, axis=1)
        current = (grouped * out_scale[depth_idx][None, :]).astype(jnp.bfloat16)
    return current
```

```python
import functools

import jax
import jax.numpy as jnp
from jax import lax
from jax.experimental import pallas as pl
from jax.experimental.pallas import tpu as pltpu
from jax.sharding import PartitionSpec as P

D = 4096
EPS = 1e-6
RING = 8
TP = 8
HALO = 32
MESH = pl.DeviceIdType.MESH
F32 = jnp.float32
BF16 = jnp.bfloat16

OFFS = (0, -1, 1, -2, 2, -3, 3, 4)


def message_keys():
    keys = []
    for dl in OFFS:
        for dh in OFFS:
            if (dl, dh) == (0, 0):
                continue
            last = dl if dh == 0 else dh
            for half in ("A", "B") if last == 4 else ("full",):
                keys.append((dl, dh, half))
    return {key: i for i, key in enumerate(keys)}


KEYS = message_keys()
XKEYS = {k: i for i, k in enumerate([(w, h) for w in ("p", "m", "2") for h in ("A", "B")])}
DKEYS = {k: i for i, k in enumerate([(w, h) for w in ("o", "p", "m", "2") for h in ("A", "B")])}
EKEYS = {k: i for i, k in enumerate([(w, c) for w in ("p", "m", "A", "B") for c in (0, 1)])}


def kernel(rows, width, depth_in, depth_mix,
           tok, docs, gain, w_in, w_mix, scale, out,
           W, X, N, G, T, acc, docx, masks, inv,
           load_sem, w_send, w_recv, x_send, x_recv, d_recv, e_send, e_recv, h_send, h_recv):
    ext = rows + HALO
    half_rows = ext // 2
    quarter = ext // 4
    sp, tp = lax.axis_index("sp"), lax.axis_index("tp")
    core = lax.rem(tp, 2)
    z, y = sp // RING, lax.rem(sp, RING)
    sps = RING * RING

    def at(dl, dh):
        ay = dl + core * (dh - dl)
        az = dh + core * (dl - dh)
        return lax.rem(z + az + RING, RING) * RING + lax.rem(y + ay + RING, RING)

    partner = tp + 1 - 2 * core
    x_plus, x_minus, x_two = lax.rem(tp + 2, TP), lax.rem(tp + TP - 2, TP), lax.rem(tp + 4, TP)
    nxt, prv = lax.rem(sp + 1, sps), lax.rem(sp + sps - 1, sps)
    light = {1: at(1, 0), -1: at(-1, 0)}
    heavy = {1: at(0, 1), -1: at(0, -1)}
    me = (sp, tp)

    own = sp
    loads = []
    for layer in range(2):
        loads.append(pltpu.make_async_copy(w_in.at[layer], W.at[layer, own, pl.ds(0, depth_in)], load_sem.at[2 * layer]))
        loads.append(pltpu.make_async_copy(w_mix.at[layer], W.at[layer, own, pl.ds(depth_in, depth_mix)], load_sem.at[2 * layer + 1]))
    loads.append(pltpu.make_async_copy(tok, X.at[0, tp, pl.ds(HALO, rows)], load_sem.at[4]))
    for c in loads:
        c.start()

    barrier = pltpu.get_barrier_semaphore()
    neighbours = [(light[1], tp), (light[-1], tp), (heavy[1], tp), (heavy[-1], tp), (nxt, tp), (prv, tp),
                  (sp, x_plus), (sp, x_minus), (sp, partner)]
    for n in neighbours:
        pl.semaphore_signal(barrier, inc=1, device_id=n, device_id_type=MESH)
    pl.semaphore_wait(barrier, len(neighbours))
    for c in loads:
        c.wait()

    def piece(r, dl, dh, half):
        ref = W.at[r, at(dl, dh)]
        if half == "A":
            return ref.at[:, pl.ds(0, width // 2)]
        if half == "B":
            return ref.at[:, pl.ds(width // 2, width // 2)]
        return ref

    def w_copy(r, dl, dh, half, key, device):
        ref = piece(r, dl, dh, half)
        return pltpu.make_async_remote_copy(ref, ref, w_send.at[r], w_recv.at[r, KEYS[key]],
                                            device_id=(device, tp), device_id_type=MESH)

    def w_wait(r, dl, dh):
        last = dl if dh == 0 else dh
        for half in ("A", "B") if last == 4 else ("full",):
            w_copy(r, dl, dh, half, (dl, dh, half), sp).wait_recv()

    def onward(r, dl, dh, axis):
        d = dl if axis == "l" else dh
        targets = light if axis == "l" else heavy
        ways = (1, -1) if d == 0 else ((1,) if d < 0 else (-1,))
        for way in ways:
            if d == 4:
                continue
            new = d - way
            half = "full"
            if abs(new) == 4:
                half, new = ("A" if way == 1 else "B"), 4
            key = (new, dh, half) if axis == "l" else (dl, new, half)
            w_copy(r, dl, dh, half, key, targets[way]).start()

    def wave(r, n):
        if n == 0:
            onward(r, 0, 0, "l")
            onward(r, 0, 0, "h")
            return
        for dl in OFFS:
            k = n - abs(dl)
            if k < 0 or k > 4:
                continue
            for dh in (0,) if k == 0 else ((4,) if k == 4 else (-k, k)):
                w_wait(r, dl, dh)
                if dh == 0:
                    onward(r, dl, 0, "l")
                    onward(r, dl, 0, "h")
                else:
                    onward(r, dl, dh, "h")

    span = {"A": pl.ds(0, half_rows), "B": pl.ds(half_rows, half_rows)}
    block_of = {"o": tp, "p": x_minus, "m": x_plus, "2": x_two}
    p_block_of = {"o": partner, "p": lax.rem(partner + TP - 2, TP), "m": lax.rem(partner + 2, TP), "2": lax.rem(partner + 4, TP)}

    def x_copy(l, who, h, key, device):
        ref = X.at[l, block_of[who], span[h]]
        return pltpu.make_async_remote_copy(ref, ref, x_send.at[l], x_recv.at[l, XKEYS[key]], device_id=(sp, device), device_id_type=MESH)

    def d_copy(l, who, h):
        ref = X.at[l, block_of[who], span[h]]
        return pltpu.make_async_remote_copy(ref, ref, x_send.at[l], d_recv.at[l, DKEYS[(who, h)]], device_id=(sp, partner), device_id_type=MESH)

    def x_own(l, h):
        x_copy(l, "o", h, ("p", h), x_plus).start()
        x_copy(l, "o", h, ("m", h), x_minus).start()
        d_copy(l, "o", h).start()

    def x_get(l, who, h):
        x_copy(l, who, h, (who, h), tp).wait_recv()
        if who == "p" and h == "A":
            x_copy(l, "p", h, ("2", h), x_plus).start()
        if who == "m" and h == "B":
            x_copy(l, "m", h, ("2", h), x_minus).start()
        d_copy(l, who, h).start()

    def d_get(l):
        for who, h in DKEYS:
            ref = X.at[l, p_block_of[who], span[h]]
            pltpu.make_async_remote_copy(ref, ref, x_send.at[l], d_recv.at[l, DKEYS[(who, h)]], device_id=me, device_id_type=MESH).wait_recv()

    half = tp // (TP // 2)
    x_plus_half = x_plus // (TP // 2)
    x_minus_half = x_minus // (TP // 2)

    def e_copy(src, dst, l, key, device):
        return pltpu.make_async_remote_copy(src, dst, e_send.at[l], e_recv.at[l, EKEYS[key]], device_id=(sp, device), device_id_type=MESH)

    def e_rows(h, c):
        return pl.ds((half_rows if h == "B" else 0) + c * quarter, quarter)

    def e_own(l):
        for c in (0, 1):
            e_copy(G.at[l, half, e_rows("A", c)], T.at[l, 0, pl.ds(c * quarter, quarter)], l, ("p", c), x_plus).start()
            e_copy(G.at[l, half, e_rows("B", c)], T.at[l, 1, pl.ds(c * quarter, quarter)], l, ("m", c), x_minus).start()

    def e_pass(l):
        for c in (0, 1):
            t0 = T.at[l, 0, pl.ds(c * quarter, quarter)]
            t1 = T.at[l, 1, pl.ds(c * quarter, quarter)]
            e_copy(t0, t0, l, ("p", c), tp).wait_recv()
            e_copy(t0, G.at[l, 1 - x_plus_half, e_rows("A", c)], l, ("A", c), x_plus).start()
            e_copy(t1, t1, l, ("m", c), tp).wait_recv()
            e_copy(t1, G.at[l, 1 - x_minus_half, e_rows("B", c)], l, ("B", c), x_minus).start()

    def e_get(l):
        for c in (0, 1):
            for h in ("A", "B"):
                ref = G.at[l, 1 - half, e_rows(h, c)]
                e_copy(ref, ref, l, (h, c), tp).wait_recv()

    def make_masks():
        top = jnp.where(sp == 0, jnp.float32(-1.0), docx[pl.ds(0, HALO), :])
        docx[pl.ds(0, HALO), :] = top
        docx[pl.ds(HALO, rows), :] = docs[...]
        d = docx[...]
        row = lax.broadcasted_iota(jnp.int32, (ext, 128), 0)
        group = lax.rem(tp, 4)
        count = jnp.ones((ext, 128), F32)
        for i in range(4):
            k = 1 << i
            taken = (pltpu.roll(d, k, 0) == d) & (row >= k) & (group >= i)
            masks[i, :, :] = taken.astype(F32)
            count = count + jnp.where(taken, pltpu.roll(count, k, 0), 0.0)
        inv[...] = 1.0 / count

    step_rows = 32

    def normalize(l):
        def body(i, _):
            at_rows = pl.ds(pl.multiple_of(i * step_rows, step_rows), step_rows)
            total = jnp.zeros((step_rows, 1), F32)
            for b in range(TP):
                v = X[l, b, at_rows, :].astype(F32)
                total = total + jnp.sum(v * v, axis=-1, keepdims=True)
            r = lax.rsqrt(total * (1.0 / D) + EPS)
            for b in range(TP):
                v = X[l, b, at_rows, :].astype(F32)
                N[b, at_rows, :] = (v * r * gain[pl.ds(l, 1), pl.ds(b * width, width)]).astype(BF16)
            return 0
        lax.fori_loop(0, ext // step_rows, body, 0)

    def project(l):
        acc[...] = jnp.zeros_like(acc)

        def body(b, _):
            w = W[l, pl.ds(pl.multiple_of(b * 8, 8), 8), pl.ds(0, depth_in), :].reshape(8 * depth_in, width)
            acc[...] += jnp.dot(N[b], w, preferred_element_type=F32)
            return 0
        lax.fori_loop(0, TP, body, 0)

    def pool(l):
        for cb in range(width // 128):
            cols = pl.ds(cb * 128, 128)
            p = acc[:, cols].astype(BF16).astype(F32)
            s = p
            for i in range(4):
                s = s + jnp.where(masks[i] > 0.5, pltpu.roll(s, 1 << i, 0), 0.0)
            G[l, half, :, cols] = (s * inv[...] - p).astype(BF16)

    def mix(l):
        a = jnp.dot(G[l, 0], W[l, pl.ds(0, 32), pl.ds(depth_in, depth_mix), :].reshape(32 * depth_mix, width), preferred_element_type=F32)
        acc[...] = a
        a = acc[...] + jnp.dot(G[l, 1], W[l, pl.ds(32, 32), pl.ds(depth_in, depth_mix), :].reshape(32 * depth_mix, width), preferred_element_type=F32)
        s = scale[pl.ds(l, 1), pl.ds(pl.multiple_of(tp * width, width), width)]
        return (a * s).astype(BF16)

    hx = X.at[0, tp, pl.ds(ext - HALO, HALO)]
    halo_x = pltpu.make_async_remote_copy(hx, X.at[0, tp, pl.ds(0, HALO)], h_send.at[0], h_recv.at[0], device_id=(nxt, tp), device_id_type=MESH)
    halo_d = pltpu.make_async_remote_copy(docs.at[pl.ds(rows - HALO, HALO)], docx.at[pl.ds(0, HALO)], h_send.at[1], h_recv.at[1], device_id=(nxt, tp), device_id_type=MESH)
    halo_x.start()
    wave(0, 0)
    halo_d.start()
    x_own(0, "B")
    halo_x.wait_recv()
    x_own(0, "A")
    wave(0, 1)
    wave(0, 2)
    x_get(0, "m", "B")
    x_get(0, "p", "B")
    halo_d.wait_recv()
    make_masks()
    wave(0, 3)
    x_get(0, "p", "A")
    x_get(0, "m", "A")
    wave(0, 4)
    x_get(0, "2", "A")
    x_get(0, "2", "B")
    wave(0, 5)
    wave(1, 0)
    d_get(0)
    normalize(0)
    wave(0, 6)
    wave(1, 1)
    wave(0, 7)
    wave(1, 2)
    wave(0, 8)
    project(0)
    pool(0)
    e_own(0)
    wave(1, 3)
    e_pass(0)
    wave(1, 4)
    e_get(0)
    X[1, tp, :, :] = mix(0)
    x_own(1, "A")
    x_own(1, "B")
    wave(1, 5)
    x_get(1, "p", "A")
    x_get(1, "m", "A")
    x_get(1, "m", "B")
    x_get(1, "p", "B")
    wave(1, 6)
    wave(1, 7)
    x_get(1, "2", "A")
    x_get(1, "2", "B")
    wave(1, 8)
    d_get(1)
    normalize(1)
    project(1)
    pool(1)
    e_own(1)
    e_pass(1)
    e_get(1)
    out[...] = mix(1)[HALO:, :]

    halo_x.wait_send()
    halo_d.wait_send()
    for l in range(2):
        ref = W.at[l, pl.ds(0, sps - 1)]
        pltpu.make_async_copy(ref, ref, w_send.at[l]).wait()
        ref = X.at[l, pl.ds(0, 7)]
        pltpu.make_async_copy(ref, ref, x_send.at[l]).wait()
        ref = G.at[l]
        pltpu.make_async_copy(ref, ref, e_send.at[l]).wait()


def shards(tokens, doc_ids, norm_gain, in_proj, mix_proj, out_scale):
    rows, width = tokens.shape
    depth_in, depth_mix = in_proj.shape[1], mix_proj.shape[1]
    ext = rows + HALO
    docs = jnp.broadcast_to(doc_ids.astype(F32)[:, None], (rows, 128))
    vmem, hbm = pl.BlockSpec(memory_space=pltpu.VMEM), pl.BlockSpec(memory_space=pl.ANY)
    return pl.pallas_call(
        functools.partial(kernel, rows, width, depth_in, depth_mix),
        name="mixer",
        out_shape=jax.ShapeDtypeStruct((rows, width), BF16),
        in_specs=[hbm, vmem, vmem, hbm, hbm, vmem],
        out_specs=vmem,
        scratch_shapes=[
            pltpu.VMEM((2, RING * RING, depth_in + depth_mix, width), BF16),
            pltpu.VMEM((2, TP, ext, width), BF16),
            pltpu.VMEM((TP, ext, width), BF16),
            pltpu.VMEM((2, 2, ext, width), BF16),
            pltpu.VMEM((2, 2, ext // 2, width), BF16),
            pltpu.VMEM((ext, width), F32),
            pltpu.VMEM((ext, 128), F32),
            pltpu.VMEM((4, ext, 128), F32),
            pltpu.VMEM((ext, 128), F32),
            pltpu.SemaphoreType.DMA((5,)),
            pltpu.SemaphoreType.DMA((2,)),
            pltpu.SemaphoreType.DMA((2, len(KEYS))),
            pltpu.SemaphoreType.DMA((2,)),
            pltpu.SemaphoreType.DMA((2, len(XKEYS))),
            pltpu.SemaphoreType.DMA((2, len(DKEYS))),
            pltpu.SemaphoreType.DMA((2,)),
            pltpu.SemaphoreType.DMA((2, len(EKEYS))),
            pltpu.SemaphoreType.DMA((2,)),
            pltpu.SemaphoreType.DMA((2,)),
        ],
        compiler_params=pltpu.CompilerParams(collective_id=0, has_side_effects=True, vmem_limit_bytes=60 * 1024 * 1024),
    )(tokens, docs, norm_gain, in_proj, mix_proj, out_scale)


def solution(mesh):
    placed = (P("sp", "tp"), P("sp"), P(), P(None, "sp", "tp"), P(None, "sp", "tp"), P())
    return jax.shard_map(
        shards, mesh=mesh, in_specs=placed, out_specs=P("sp", "tp"), check_vma=False
    )
```

```python
import functools

import jax
import jax.numpy as jnp
from jax import lax
from jax.experimental import pallas as pl
from jax.experimental.pallas import tpu as pltpu
from jax.sharding import PartitionSpec as P

D = 4096
EPS = 1e-6
RING = 8
TP = 8
HALO = 32
MESH = pl.DeviceIdType.MESH
F32 = jnp.float32
BF16 = jnp.bfloat16
OUT = BF16

RATE, X_RATE, D_RATE = 92.0, 46.0, 560.0
HOP, X_HOP, D_HOP, DT = 2.8, 2.4, 1.6, 0.05
OFFS = (0, -1, 1, -2, 2, -3, 3, 4)
ROUNDS = ((0, 0), (0, 1), (1, 0), (1, 1))
BASE, STEP = (0, 2.6, 10, 12.6), (1, 1, 1, 1)
LIMIT = 0.4
PIECE_ROWS = (64, 16, 80)
SHARE = ((0, 1, 2, 3, 4), (0, 0, 0, 0, 0), (0, 1, 2, 3, 4))
GATHER = (((0, 96), (96, 64), (160, 80), (240, 80)), ((16, 80), (96, 64), (160, 80), (240, 80)))
EXCHANGE = (GATHER[1], ((32, 64), (96, 80), (176, 64), (240, 80)))
WINDOWS = (((0, 320),), ((16, 80), (80, 96), (160, 80), (224, 96)))
WINDOW_OF = ((0, 0, 0, 0), (0, 1, 2, 3))
WINDOW_NEEDS = (((0, 1, 2, 3),), ((0,), (0, 1, 2), (2,), (2, 3)))
TIME = {"project": 2.3, "mix": 0.4, "norm": 0.7, "masks": 0.3, "halo": 0.1}
EARLY = {("norm", 0): 19.0}


def halves(last):
    return ("A", "B") if last == 4 else ("full",)


def message_groups():
    groups = []
    for _, kind in ROUNDS:
        members = {}
        for dl in OFFS:
            for dh in OFFS:
                for half in halves(dl if dh == 0 else dh) if (dl, dh) != (0, 0) else ():
                    name = (dl, 0, half) if dh == 0 else (SHARE[kind][abs(dl)], dh, half, "h")
                    members.setdefault(name, []).append((dl, dh, half))
        groups.append(list(members.values()))
    return groups, [{key: i for i, keys in enumerate(g) for key in keys} for g in groups]


GROUPS, GROUP_OF = message_groups()


def build():
    rate = {"hF": RATE, "hB": RATE, "lF": RATE, "lB": RATE, "xF": X_RATE, "xB": X_RATE, "d": D_RATE}
    hops = {"x": X_HOP, "d": D_HOP}
    items, tasks = [], []

    def send(flow, kb, need, prio, gives, op):
        items.append([flow, kb, need, prio, gives, op])

    def task(need, op, gives, prio, time=None):
        tasks.append([need, time or TIME[op[0]], op, gives, prio])

    def all_pieces(layer, kind):
        return [("w", r, a, b, h) for r, round in enumerate(ROUNDS) if round[0] == layer and round[1] in (kind, 2)
                for a in OFFS for b in OFFS if (a, b) != (0, 0) for h in halves(a if b == 0 else b)]
    for r, (_, kind) in enumerate(ROUNDS):
        kb = PIECE_ROWS[kind] * 1.024
        for dl in OFFS:
            for dh in OFFS:
                for axis in ("l", "h") if dh == 0 else ("h",):
                    d = dl if axis == "l" else dh
                    if d == 4:
                        continue
                    for way in (1, -1) if d == 0 else ((1,) if d < 0 else (-1,)):
                        new, half = d - way, "full"
                        if abs(new) == 4:
                            new, half = 4, ("A" if way == 1 else "B")
                        key = (new, 0, half) if axis == "l" else (dl, new, half)
                        prio = (BASE[r] - 0.5, abs(dl)) if axis == "l" else (BASE[r] + abs(d) * STEP[r], abs(dl))
                        need = [] if (dl, dh) == (0, 0) else [("w", r, dl, dh, h) for h in halves(dl if dh == 0 else dh)]
                        send(axis + ("F" if way == 1 else "B"), kb / len(halves(new)), need, prio, ("w", r) + key, ("ws", r, dl, dh, axis, way))
    for l in range(2):
        for c in range(4):
            own, kb, phase, side = [("cur", l, c)], GATHER[l][c][1] * 1.024, c % 2, c // 2
            send("xF", kb, own, (l, 0, phase, side), ("x", l, "p", c), ("xs", l, "o", c, 1))
            send("xB", kb, own, (l, 0, phase, 1 - side), ("x", l, "m", c), ("xs", l, "o", c, -1))
            send("d", kb, own, (l, 0, c), ("d", l, "o", c), ("ds", l, "o", c))
            way = 1 - 2 * side
            send(("xF", "xB")[side], kb, [("x", l, "pm"[side], c)], (l, 0, phase, -1), ("x", l, "2", c), ("xs", l, "pm"[side], c, way))
            for who in ("p", "m", "2"):
                send("d", kb, [("x", l, who, c)], (l, 1, c), ("d", l, who, c), ("ds", l, who, c))
            need = [("x", l, w, c) for w in ("p", "m", "2")] + [("d", l, w, c) for w in ("o", "p", "m", "2")] + own
            task(need, ("norm", l, c), [("n", l, c)], (l, 0, phase, c))
            kb = EXCHANGE[l][c][1] * 1.024
            send(("xF", "xB")[side], kb, [("pool", l, WINDOW_OF[l][c])], (l, 1, phase, 0), ("t", l, c), ("es", l, c))
            send(("xF", "xB")[side], kb, [("t", l, c)], (l, 1, phase, -1), ("e", l, c), ("ep", l, c))
            task([("e", l, c), ("pool", l, WINDOW_OF[l][c])] + all_pieces(l, 1), ("mix", l, c), [("cur", l + 1, c)], (l, 2, phase, c))
        for w, needs in enumerate(WINDOW_NEEDS[l]):
            task(all_pieces(l, 0) + [("n", l, c) for c in needs] + [("masks",)], ("project", l, w), [("pool", l, w)], (l, 1, w % 2, w), (2.3, 1.2)[l])
    task([("halo",)], ("halo",), [("cur", 0, 0)], (-1, 0, 0, 0))
    task([("halo",)], ("masks",), [("masks",)], (0, -1, 0, 0))
    have = {("cur", 0, c): 0.0 for c in range(1, 4)}
    arrivals, finishing, landed = [(3.0, ("halo",))], [], {}
    flows = {f: [] for f in rate}
    ops, t, busy, done_at = [], 0.0, 0.0, {}
    items.sort(key=lambda i: i[3])
    tasks.sort(key=lambda k: k[4])
    while items or tasks:
        for a in [a for a in arrivals if a[0] <= t + 1e-9]:
            arrivals.remove(a)
            if a[1][0] == "w":
                r, group = a[1][1], (a[1][1], GROUP_OF[a[1][1]][a[1][2:]])
                landed[group] = landed.get(group, 0) + 1
                if landed[group] == len(GROUPS[r][group[1]]):
                    have.update({("w", r) + key: a[0] for key in GROUPS[r][group[1]]})
            else:
                have[a[1]] = a[0]
        for a in [a for a in finishing if a[0] <= t + 1e-9]:
            finishing.remove(a)
            for g in a[1]:
                have[g] = t
        if t >= busy - 1e-9:
            again = True
            while again:
                again = False
                for i in items:
                    f = i[0]
                    if sum(x[1] for x in flows[f]) / rate[f] <= LIMIT and all(n in have for n in i[2]):
                        items.remove(i)
                        flows[f].append([i, i[1]])
                        ops.append((t, i[5], i[2]))
                        again = True
                        break
            for k in tasks:
                if t >= EARLY.get(k[2][:2], 0.0) and all(n in have for n in k[0]):
                    tasks.remove(k)
                    ops.append((t, k[2], k[0]))
                    busy = t + k[1]
                    finishing.append((busy, k[3]))
                    done_at[k[2]] = busy
                    break
        active = {f: bool(flows[f]) for f in flows}
        for f in flows:
            share = 1.0 / (active["h" + f[1]] + active["l" + f[1]]) if active[f] and f[0] in "hl" else 1.0
            left = rate[f] * share * DT
            while flows[f] and left > 0:
                q = flows[f][0]
                use = min(left, q[1])
                q[1] -= use
                left -= use
                if q[1] <= 1e-9:
                    flows[f].pop(0)
                    arrivals.append((t + DT + hops.get(f[0], HOP), q[0][4]))
        t += DT
    return ops, done_at, have


FIRST = [sum(len(g) for g in GROUPS[:r]) for r in range(len(ROUNDS) + 1)]
WHO = {"p": 0, "m": 1, "2": 2, "o": 3}


def kernel(rows, width, depth_in, depth_mix,
           tok, docs_in, gain_in, w_in, w_mix, scale_in, out_hbm,
           W, X, N, G, T, acc, docx, masks, inv, docs, gain, scale, out,
           load_sem, w_send, w_recv, x_send, x_recv, d_recv, e_send, t_recv, e_recv, h_send, h_recv, o_send):
    ext = rows + HALO
    sp, tp = lax.axis_index("sp"), lax.axis_index("tp")
    core = lax.rem(tp, 2)
    z, y = sp // RING, lax.rem(sp, RING)
    sps = RING * RING

    def at(dl, dh):
        ay = dl + core * (dh - dl)
        az = dh + core * (dl - dh)
        return lax.rem(z + az + RING, RING) * RING + lax.rem(y + ay + RING, RING)

    partner = tp + 1 - 2 * core
    x_plus, x_minus, x_two = lax.rem(tp + 2, TP), lax.rem(tp + TP - 2, TP), lax.rem(tp + 4, TP)
    nxt, prv = lax.rem(sp + 1, sps), lax.rem(sp + sps - 1, sps)
    target = {("l", 1): at(1, 0), ("l", -1): at(-1, 0), ("h", 1): at(0, 1), ("h", -1): at(0, -1)}
    me = (sp, tp)

    barrier = pltpu.get_barrier_semaphore()
    neighbours = [(d, tp) for d in target.values()] + [(nxt, tp), (prv, tp), (sp, x_plus), (sp, x_minus), (sp, partner)]
    for n in neighbours:
        pl.semaphore_signal(barrier, inc=1, device_id=n, device_id_type=MESH)

    def spread_docs():
        for k in range(0, rows, 128):
            n = min(128, rows - k)
            line = docs[pl.ds(k, n)].astype(F32).reshape(1, n)
            if n < 128:
                line = jnp.concatenate([line, jnp.zeros((1, 128 - n), F32)], axis=1)
            docx[pl.ds(HALO + k, n), :] = jnp.transpose(jnp.broadcast_to(line, (128, 128)))[:n, :]

    weight_rows = (pl.ds(0, depth_in), pl.ds(depth_in, depth_mix), pl.ds(0, depth_in + depth_mix))
    small = [pltpu.make_async_copy(docs_in, docs, load_sem.at[5]), pltpu.make_async_copy(gain_in, gain, load_sem.at[6]), pltpu.make_async_copy(scale_in, scale, load_sem.at[7])]
    loads = [pltpu.make_async_copy(tok, X.at[0, tp, pl.ds(HALO, rows)], load_sem.at[4])]
    for layer in range(2):
        for is_mix in range(2):
            loads.append(pltpu.make_async_copy((w_in, w_mix)[is_mix].at[layer], W.at[layer, sp, weight_rows[is_mix]], load_sem.at[2 * layer + is_mix]))
    for c in small[:1] + loads + small[1:]:
        c.start()
    small[0].wait()
    spread_docs()
    for c in loads + small[1:]:
        c.wait()
    pl.semaphore_wait(barrier, len(neighbours))

    def w_copy(r, dl, dh, half, key, device):
        layer, which = ROUNDS[r]
        ref = W.at[layer, at(dl, dh), weight_rows[which]]
        if half != "full":
            ref = ref.at[:, pl.ds(0 if half == "A" else width // 2, width // 2)]
        return pltpu.make_async_remote_copy(ref, ref, w_send.at[r], w_recv.at[FIRST[r] + GROUP_OF[r][key]], device_id=(device, tp), device_id_type=MESH)

    def onward(r, dl, dh, axis, way):
        new, half = (dl if axis == "l" else dh) - way, "full"
        if abs(new) == 4:
            new, half = 4, ("A" if way == 1 else "B")
        key = (new, 0, half) if axis == "l" else (dl, new, half)
        w_copy(r, dl, dh, half, key, target[axis, way]).start()

    def span(chunk):
        return pl.ds(*chunk)

    def blocks(first):
        return {"o": first, "p": lax.rem(first + TP - 2, TP), "m": lax.rem(first + 2, TP), "2": lax.rem(first + 4, TP)}

    block_of, partner_block_of = blocks(tp), blocks(partner)

    def x_copy(l, who, c, key, device):
        ref = X.at[l, block_of[who], span(GATHER[l][c])]
        return pltpu.make_async_remote_copy(ref, ref, x_send.at[l], x_recv.at[l, WHO[key] * 4 + c], device_id=(sp, device), device_id_type=MESH)

    def d_copy(l, block, who, c):
        ref = X.at[l, block[who], span(GATHER[l][c])]
        return pltpu.make_async_remote_copy(ref, ref, x_send.at[l], d_recv.at[l, WHO[who] * 4 + c], device_id=(sp, partner), device_id_type=MESH)

    half_of = tp // (TP // 2)

    def t_copy(l, c, device):
        rows_of = span(EXCHANGE[l][c])
        return pltpu.make_async_remote_copy(G.at[l, half_of, rows_of], T.at[l, rows_of], e_send.at[l], t_recv.at[l, c], device_id=(sp, device), device_id_type=MESH)

    def e_copy(l, c, device):
        rows_of, slot = span(EXCHANGE[l][c]), 1 - device // (TP // 2)
        return pltpu.make_async_remote_copy(T.at[l, rows_of], G.at[l, slot, rows_of], e_send.at[l], e_recv.at[l, c], device_id=(sp, device), device_id_type=MESH)

    def make_masks():
        docx[pl.ds(0, HALO), :] = jnp.where(sp == 0, jnp.float32(-1.0), docx[pl.ds(0, HALO), :])
        d = docx[...]
        row = lax.broadcasted_iota(jnp.int32, (ext, 128), 0)
        group = lax.rem(tp, 4)
        count = jnp.ones((ext, 128), F32)
        for i in range(4):
            k = 1 << i
            taken = (pltpu.roll(d, k, 0) == d) & (row >= k) & (group >= i)
            masks[i, :, :] = taken.astype(F32)
            count = count + jnp.where(taken, pltpu.roll(count, k, 0), 0.0)
        inv[...] = 1.0 / count

    step_rows = 16

    def normalize(l, c):
        def body(i, _):
            at_rows = pl.ds(pl.multiple_of(GATHER[l][c][0] + i * step_rows, step_rows), step_rows)
            total = jnp.zeros((step_rows, 1), F32)
            for b in range(TP):
                v = X[l, b, at_rows, :].astype(F32)
                total = total + jnp.sum(v * v, axis=-1, keepdims=True)
            r = lax.rsqrt(total * (1.0 / D) + EPS)
            for b in range(TP):
                v = X[l, b, at_rows, :].astype(F32)
                N[at_rows, pl.ds(b * width, width)] = (v * r * gain[pl.ds(l, 1), pl.ds(b * width, width)]).astype(BF16)
            return 0
        lax.fori_loop(0, GATHER[l][c][1] // step_rows, body, 0)

    def project(l, window):
        first, n = WINDOWS[l][window]
        w = W[l, :, pl.ds(0, depth_in), :].reshape(sps * depth_in, width)
        acc[pl.ds(0, n), :] = jnp.dot(N[pl.ds(first, n), :], w, preferred_element_type=F32)
        for cb in range(width // 128):
            cols = pl.ds(cb * 128, 128)
            p = acc[pl.ds(0, n), cols].astype(BF16).astype(F32)
            s = p
            for i in range(4):
                s = s + jnp.where(masks[i, pl.ds(first, n), :] > 0.5, pltpu.roll(s, 1 << i, 0), 0.0)
            pooled = (s * inv[pl.ds(first, n), :] - p).astype(BF16)
            G[l, half_of, pl.ds(first + 16, n - 16), cols] = pooled[16:, :]

    def mix(l, c):
        first, n = EXCHANGE[l][c]
        a = jnp.zeros((n, width), F32)
        for h in range(2):
            w = W[l, pl.ds(h * (sps // 2), sps // 2), pl.ds(depth_in, depth_mix), :].reshape(sps // 2 * depth_mix, width)
            a = a + jnp.dot(G[l, h, pl.ds(first, n), :], w, preferred_element_type=F32)
        a = a * scale[pl.ds(l, 1), pl.ds(pl.multiple_of(tp * width, width), width)]
        if l == 0:
            X[1, tp, pl.ds(first, n), :] = a.astype(BF16)
        else:
            rows_of = pl.ds(first - HALO, n)
            out[rows_of, :] = a.astype(out.dtype)
            pltpu.make_async_copy(out.at[rows_of], out_hbm.at[rows_of], o_send.at[c]).start()

    halo_x = pltpu.make_async_remote_copy(X.at[0, tp, pl.ds(ext - HALO, HALO)], X.at[0, tp, pl.ds(0, HALO)], h_send.at[0], h_recv.at[0], device_id=(nxt, tp), device_id_type=MESH)
    halo_d = pltpu.make_async_remote_copy(docx.at[pl.ds(rows, HALO)], docx.at[pl.ds(0, HALO)], h_send.at[1], h_recv.at[1], device_id=(nxt, tp), device_id_type=MESH)
    halo_x.start()
    halo_d.start()

    def wait(token):
        name = token[0]
        if name == "w":
            layer, which = ROUNDS[token[1]]
            keys = GROUPS[token[1]][GROUP_OF[token[1]][token[2:]]]
            ref = W.at[layer, pl.ds(0, len(keys)), weight_rows[which]]
            if token[4] != "full":
                ref = ref.at[:, :, pl.ds(0, width // 2)]
            pltpu.make_async_copy(ref, ref, w_recv.at[FIRST[token[1]] + GROUP_OF[token[1]][token[2:]]]).wait()
            waited.update(("w", token[1]) + key for key in keys)
        elif name == "x":
            l, who, c = token[1:]
            x_copy(l, who, c, who, tp).wait_recv()
        elif name == "d":
            l, who, c = token[1:]
            d_copy(l, partner_block_of, who, c).wait_recv()
        elif name == "t":
            t_copy(*token[1:], tp).wait_recv()
        elif name == "e":
            l, c = token[1:]
            ref = G.at[l, 1 - half_of, span(EXCHANGE[l][c])]
            pltpu.make_async_remote_copy(ref, ref, e_send.at[l], e_recv.at[l, c], device_id=me, device_id_type=MESH).wait_recv()
        elif name == "halo":
            halo_x.wait_recv()
            halo_d.wait_recv()

    x_way = {1: x_plus, -1: x_minus}
    waited = set()
    ops, _, _ = build()
    for _, op, need in ops:
        for token in need:
            if token not in waited:
                waited.add(token)
                wait(token)
        name = op[0]
        if name == "ws":
            onward(*op[1:])
        elif name == "xs":
            l, who, c, way = op[1:]
            x_copy(l, who, c, {"o": "p" if way == 1 else "m"}.get(who, "2"), x_way[way]).start()
        elif name == "ds":
            d_copy(op[1], block_of, op[2], op[3]).start()
        elif name == "es":
            t_copy(*op[1:], x_way[1 if op[2] < 2 else -1]).start()
        elif name == "ep":
            e_copy(*op[1:], x_way[1 if op[2] < 2 else -1]).start()
        elif name == "norm":
            normalize(op[1], op[2])
        elif name == "project":
            project(op[1], op[2])
        elif name == "mix":
            mix(op[1], op[2])
        elif name == "masks":
            make_masks()

    for c, (first, n) in enumerate(EXCHANGE[1]):
        rows_of = pl.ds(first - HALO, n)
        pltpu.make_async_copy(out.at[rows_of], out_hbm.at[rows_of], o_send.at[c]).wait()
    halo_x.wait_send()
    halo_d.wait_send()
    for r, (layer, which) in enumerate(ROUNDS):
        ref = W.at[layer, pl.ds(0, sps - 1), weight_rows[which]]
        pltpu.make_async_copy(ref, ref, w_send.at[r]).wait()
    for l in range(2):
        ref = X.at[l, pl.ds(0, 7), pl.ds(0, ext - l * HALO // 2)]
        pltpu.make_async_copy(ref, ref, x_send.at[l]).wait()
        ref = G.at[l, :, pl.ds(0, ext - (l + 1) * HALO // 2)]
        pltpu.make_async_copy(ref, ref, e_send.at[l]).wait()


def shards(tokens, doc_ids, norm_gain, in_proj, mix_proj, out_scale):
    rows, width = tokens.shape
    depth_in, depth_mix = in_proj.shape[1], mix_proj.shape[1]
    ext = rows + HALO
    docs = doc_ids
    hbm = pl.BlockSpec(memory_space=pl.ANY)
    dma = pltpu.SemaphoreType.DMA
    return pl.pallas_call(
        functools.partial(kernel, rows, width, depth_in, depth_mix),
        name="mixer",
        out_shape=jax.ShapeDtypeStruct((rows, width), OUT),
        in_specs=[hbm] * 6,
        out_specs=hbm,
        scratch_shapes=[
            pltpu.VMEM((2, RING * RING, depth_in + depth_mix, width), BF16),
            pltpu.VMEM((2, TP, ext, width), BF16),
            pltpu.VMEM((ext, D), BF16),
            pltpu.VMEM((2, 2, ext, width), BF16),
            pltpu.VMEM((2, ext, width), BF16),
            pltpu.VMEM((ext, width), F32),
            pltpu.VMEM((ext, 128), F32),
            pltpu.VMEM((4, ext, 128), F32),
            pltpu.VMEM((ext, 128), F32),
            pltpu.VMEM((rows,), jnp.int32),
            pltpu.VMEM((2, D), F32),
            pltpu.VMEM((2, D), F32),
            pltpu.VMEM((rows, width), OUT),
            dma((8,)),
            dma((len(ROUNDS),)),
            dma((FIRST[-1],)),
            dma((2,)),
            dma((2, 12)),
            dma((2, 16)),
            dma((2,)),
            dma((2, 4)),
            dma((2, 4)),
            dma((2,)),
            dma((2,)),
            dma((4,)),
        ],
        compiler_params=pltpu.CompilerParams(collective_id=0, has_side_effects=True, vmem_limit_bytes=60 * 1024 * 1024),
    )(tokens, docs, norm_gain, in_proj, mix_proj, out_scale)


def solution(mesh):
    placed = (P("sp", "tp"), P("sp"), P(), P(None, "sp", "tp"), P(None, "sp", "tp"), P())
    return jax.shard_map(
        shards, mesh=mesh, in_specs=placed, out_specs=P("sp", "tp"), check_vma=False
    )
```

```python
import functools

import jax
import jax.numpy as jnp
from jax import lax
from jax.experimental import pallas as pl
from jax.experimental.pallas import tpu as pltpu
from jax.sharding import PartitionSpec as P

D = 4096
EPS = 1e-6
RING = 8
TP = 8
HALO = 32
MESH = pl.DeviceIdType.MESH
F32 = jnp.float32
BF16 = jnp.bfloat16

RATE, X_RATE, D_RATE = 92.0, 46.0, 560.0
HOP, X_HOP, D_HOP, DT = 2.8, 2.4, 1.6, 0.05
OFFS = (0, -1, 1, -2, 2, -3, 3, 4)
ROUNDS = ((0, 0), (0, 1), (1, 0), (1, 1))
BASE, STEP = (0, 2.6, 10, 12.6), (1, 1, 1, 1)
LIMIT = 0.4
STRAIGHT = (1,)
ROUTED = 0.75
PIECE_ROWS = (64, 16, 80)
SHARE = ((0, 1, 2, 3, 4), (0, 0, 0, 0, 0), (0, 1, 2, 3, 4))
GATHER = (((0, 112), (112, 48), (160, 96), (256, 64)), ((16, 96), (112, 48), (160, 96), (256, 64)))
EXCHANGE = (GATHER[1], ((32, 80), (112, 64), (176, 80), (256, 64)))
WINDOWS = (((0, 320),), ((16, 96), (96, 80), (160, 96), (240, 80)))
WINDOW_OF = ((0, 0, 0, 0), (0, 1, 2, 3))
WINDOW_NEEDS = (((0, 1, 2, 3),), ((0,), (0, 1, 2), (2,), (2, 3)))
TIME = {"project": 2.3, "mix": 0.4, "norm": 0.7, "masks": 0.3, "halo": 0.1}
EARLY = {("norm", 0): 19.0}


def halves(last):
    return ("A", "B") if last == 4 else ("full",)


def message_groups():
    groups = []
    for _, kind in ROUNDS:
        members = {}
        for dl in OFFS:
            for dh in OFFS:
                for half in halves(dl if dh == 0 else dh) if (dl, dh) != (0, 0) else ():
                    name = (dl, 0, half) if dh == 0 else (SHARE[kind][abs(dl)], dh, half, "h")
                    members.setdefault(name, []).append((dl, dh, half))
        groups.append(list(members.values()))
    return groups, [{key: i for i, keys in enumerate(g) for key in keys} for g in groups]


GROUPS, GROUP_OF = message_groups()


def build():
    rate = {"hF": RATE, "hB": RATE, "lF": RATE, "lB": RATE, "xF": X_RATE, "xB": X_RATE, "d": D_RATE}
    hops = {"x": X_HOP, "d": D_HOP}
    items, tasks = [], []

    def send(flow, kb, need, prio, gives, op):
        items.append([flow, kb, need, prio, gives, op])

    def task(need, op, gives, prio, time=None):
        tasks.append([need, time or TIME[op[0]], op, gives, prio])

    def all_pieces(layer, kind):
        return [("w", r, a, b, h) for r, round in enumerate(ROUNDS) if round[0] == layer and round[1] in (kind, 2)
                for a in OFFS for b in OFFS if (a, b) != (0, 0) for h in halves(a if b == 0 else b)]
    for r, (_, kind) in enumerate(ROUNDS):
        kb = PIECE_ROWS[kind] * 1.024
        for dl in OFFS:
            for dh in OFFS:
                for axis in ("l", "h") if dh == 0 else ("h",):
                    d = dl if axis == "l" else dh
                    if d == 4:
                        continue
                    for way in (1, -1) if d == 0 else ((1,) if d < 0 else (-1,)):
                        new, half = d - way, "full"
                        if abs(new) == 4:
                            new, half = 4, ("A" if way == 1 else "B")
                        key = (new, 0, half) if axis == "l" else (dl, new, half)
                        prio = (BASE[r] - 0.5, abs(dl)) if axis == "l" else (BASE[r] + abs(d) * STEP[r], abs(dl))
                        need = [] if (dl, dh) == (0, 0) else [("w", r, dl, dh, h) for h in halves(dl if dh == 0 else dh)]
                        send(axis + ("F" if way == 1 else "B"), kb / len(halves(new)), need, prio, ("w", r) + key, ("ws", r, dl, dh, axis, way))
    for l in range(2):
        for c in range(4):
            own, kb, phase, side = [("cur", l, c)], GATHER[l][c][1] * 1.024, c % 2, c // 2
            send("xF", kb, own, (l, 0, phase, side), ("x", l, "p", c), ("xs", l, "o", c, 1))
            send("xB", kb, own, (l, 0, phase, 1 - side), ("x", l, "m", c), ("xs", l, "o", c, -1))
            send("d", kb, own, (l, 0, c), ("d", l, "o", c), ("ds", l, "o", c))
            way = 1 - 2 * side
            send(("xF", "xB")[side], kb, [("x", l, "pm"[side], c)], (l, 0, phase, -1), ("x", l, "2", c), ("xs", l, "pm"[side], c, way))
            for who in ("p", "m", "2"):
                send("d", kb, [("x", l, who, c)], (l, 1, c), ("d", l, who, c), ("ds", l, who, c))
            need = [("x", l, w, c) for w in ("p", "m", "2")] + [("d", l, w, c) for w in ("o", "p", "m", "2")] + own
            task(need, ("norm", l, c), [("n", l, c)], (l, 0, phase, c))
            kb = EXCHANGE[l][c][1] * 1.024
            if l in STRAIGHT:
                send(("xF", "xB")[side], 2 * kb, [("pool", l, WINDOW_OF[l][c])], (l, 1, phase, 0), ("e", l, c), ("ed", l, c))
            else:
                send(("xF", "xB")[side], kb, [("pool", l, WINDOW_OF[l][c])], (l, 1, phase, 0), ("t", l, c), ("es", l, c))
                send(("xF", "xB")[side], kb, [("t", l, c)], (l, 1, phase, -1), ("e", l, c), ("ep", l, c))
            task([("e", l, c), ("pool", l, WINDOW_OF[l][c])] + all_pieces(l, 1), ("mix", l, c), [("cur", l + 1, c)], (l, 2, phase, c))
        for w, needs in enumerate(WINDOW_NEEDS[l]):
            task(all_pieces(l, 0) + [("n", l, c) for c in needs] + [("masks",)], ("project", l, w), [("pool", l, w)], (l, 1, w % 2, w), (2.3, 1.0)[l])
    task([("halo",)], ("halo",), [("cur", 0, 0)], (-1, 0, 0, 0))
    task([("halo",)], ("masks",), [("masks",)], (0, -1, 0, 0))
    have = {("cur", 0, c): 0.0 for c in range(1, 4)}
    arrivals, finishing, landed = [(3.0, ("halo",))], [], {}
    flows = {f: [] for f in rate}
    ops, t, busy, done_at = [], 0.0, 0.0, {}
    items.sort(key=lambda i: i[3])
    tasks.sort(key=lambda k: k[4])
    while items or tasks:
        for a in [a for a in arrivals if a[0] <= t + 1e-9]:
            arrivals.remove(a)
            if a[1][0] == "w":
                r, group = a[1][1], (a[1][1], GROUP_OF[a[1][1]][a[1][2:]])
                landed[group] = landed.get(group, 0) + 1
                if landed[group] == len(GROUPS[r][group[1]]):
                    have.update({("w", r) + key: a[0] for key in GROUPS[r][group[1]]})
            else:
                have[a[1]] = a[0]
        for a in [a for a in finishing if a[0] <= t + 1e-9]:
            finishing.remove(a)
            for g in a[1]:
                have[g] = t
        if t >= busy - 1e-9:
            again = True
            while again:
                again = False
                for i in items:
                    f = i[0]
                    if sum(x[1] for x in flows[f]) / rate[f] <= LIMIT and all(n in have for n in i[2]):
                        items.remove(i)
                        flows[f].append([i, i[1]])
                        ops.append((t, i[5], i[2]))
                        again = True
                        break
            for k in tasks:
                if t >= EARLY.get(k[2][:2], 0.0) and all(n in have for n in k[0]):
                    tasks.remove(k)
                    ops.append((t, k[2], k[0]))
                    busy = t + k[1]
                    finishing.append((busy, k[3]))
                    done_at[k[2]] = busy
                    break
        active = {f: bool(flows[f]) for f in flows}
        for f in flows:
            share = 1.0 / (active["h" + f[1]] + active["l" + f[1]]) if active[f] and f[0] in "hl" else 1.0
            left = rate[f] * share * DT
            while flows[f] and left > 0:
                q = flows[f][0]
                use = min(left, q[1])
                q[1] -= use
                left -= use
                if q[1] <= 1e-9:
                    flows[f].pop(0)
                    arrivals.append((t + DT + hops.get(f[0], HOP) + (ROUTED if q[0][5][0] == "ed" else 0.0), q[0][4]))
        t += DT
    return ops, done_at, have


FIRST = [sum(len(g) for g in GROUPS[:r]) for r in range(len(ROUNDS) + 1)]
WHO = {"p": 0, "m": 1, "2": 2, "o": 3}


def kernel(rows, width, depth_in, depth_mix,
           tok, docs_in, gain_in, w_in, w_mix, scale_in, out,
           W, X, N, G, T, acc, docx, masks, inv, docs, gain, scale,
           load_sem, w_send, w_recv, x_send, x_recv, d_recv, e_send, t_recv, e_recv, h_send, h_recv):
    ext = rows + HALO
    sp, tp = lax.axis_index("sp"), lax.axis_index("tp")
    core = lax.rem(tp, 2)
    z, y = sp // RING, lax.rem(sp, RING)
    sps = RING * RING

    def at(dl, dh):
        ay = dl + core * (dh - dl)
        az = dh + core * (dl - dh)
        return lax.rem(z + az + RING, RING) * RING + lax.rem(y + ay + RING, RING)

    partner = tp + 1 - 2 * core
    x_plus, x_minus, x_two = lax.rem(tp + 2, TP), lax.rem(tp + TP - 2, TP), lax.rem(tp + 4, TP)
    nxt, prv = lax.rem(sp + 1, sps), lax.rem(sp + sps - 1, sps)
    target = {("l", 1): at(1, 0), ("l", -1): at(-1, 0), ("h", 1): at(0, 1), ("h", -1): at(0, -1)}
    me = (sp, tp)

    barrier = pltpu.get_barrier_semaphore()
    neighbours = [(d, tp) for d in target.values()] + [(nxt, tp), (prv, tp), (sp, x_plus), (sp, x_minus), (sp, x_two), (sp, partner)]
    for n in neighbours:
        pl.semaphore_signal(barrier, inc=1, device_id=n, device_id_type=MESH)

    def spread_docs():
        for k in range(0, rows, 128):
            n = min(128, rows - k)
            line = docs[pl.ds(k, n)].astype(F32).reshape(1, n)
            if n < 128:
                line = jnp.concatenate([line, jnp.zeros((1, 128 - n), F32)], axis=1)
            docx[pl.ds(HALO + k, n), :] = jnp.transpose(jnp.broadcast_to(line, (128, 128)))[:n, :]

    weight_rows = (pl.ds(0, depth_in), pl.ds(depth_in, depth_mix), pl.ds(0, depth_in + depth_mix))
    small = [pltpu.make_async_copy(docs_in, docs, load_sem.at[5]), pltpu.make_async_copy(gain_in, gain, load_sem.at[6]), pltpu.make_async_copy(scale_in, scale, load_sem.at[7])]
    loads = [pltpu.make_async_copy(tok, X.at[0, tp, pl.ds(HALO, rows)], load_sem.at[4])]
    for layer in range(2):
        for is_mix in range(2):
            loads.append(pltpu.make_async_copy((w_in, w_mix)[is_mix].at[layer], W.at[layer, sp, weight_rows[is_mix]], load_sem.at[2 * layer + is_mix]))
    for c in small[:1] + loads + small[1:]:
        c.start()
    small[0].wait()
    spread_docs()
    for c in loads + small[1:]:
        c.wait()
    pl.semaphore_wait(barrier, len(neighbours))

    def w_copy(r, dl, dh, half, key, device):
        layer, which = ROUNDS[r]
        ref = W.at[layer, at(dl, dh), weight_rows[which]]
        if half != "full":
            ref = ref.at[:, pl.ds(0 if half == "A" else width // 2, width // 2)]
        return pltpu.make_async_remote_copy(ref, ref, w_send.at[r], w_recv.at[FIRST[r] + GROUP_OF[r][key]], device_id=(device, tp), device_id_type=MESH)

    def onward(r, dl, dh, axis, way):
        new, half = (dl if axis == "l" else dh) - way, "full"
        if abs(new) == 4:
            new, half = 4, ("A" if way == 1 else "B")
        key = (new, 0, half) if axis == "l" else (dl, new, half)
        w_copy(r, dl, dh, half, key, target[axis, way]).start()

    def span(chunk):
        return pl.ds(*chunk)

    def blocks(first):
        return {"o": first, "p": lax.rem(first + TP - 2, TP), "m": lax.rem(first + 2, TP), "2": lax.rem(first + 4, TP)}

    block_of, partner_block_of = blocks(tp), blocks(partner)

    def x_copy(l, who, c, key, device):
        ref = X.at[l, block_of[who], span(GATHER[l][c])]
        return pltpu.make_async_remote_copy(ref, ref, x_send.at[l], x_recv.at[l, WHO[key] * 4 + c], device_id=(sp, device), device_id_type=MESH)

    def d_copy(l, block, who, c):
        ref = X.at[l, block[who], span(GATHER[l][c])]
        return pltpu.make_async_remote_copy(ref, ref, x_send.at[l], d_recv.at[l, WHO[who] * 4 + c], device_id=(sp, partner), device_id_type=MESH)

    half_of = tp // (TP // 2)

    def t_copy(l, c, device):
        rows_of = span(EXCHANGE[l][c])
        return pltpu.make_async_remote_copy(G.at[l, half_of, rows_of], T.at[l, rows_of], e_send.at[l], t_recv.at[l, c], device_id=(sp, device), device_id_type=MESH)

    def e_copy(l, c, device):
        rows_of, slot = span(EXCHANGE[l][c]), 1 - device // (TP // 2)
        return pltpu.make_async_remote_copy(T.at[l, rows_of], G.at[l, slot, rows_of], e_send.at[l], e_recv.at[l, c], device_id=(sp, device), device_id_type=MESH)

    def make_masks():
        docx[pl.ds(0, HALO), :] = jnp.where(sp == 0, jnp.float32(-1.0), docx[pl.ds(0, HALO), :])
        d = docx[...]
        row = lax.broadcasted_iota(jnp.int32, (ext, 128), 0)
        group = lax.rem(tp, 4)
        count = jnp.ones((ext, 128), F32)
        for i in range(4):
            k = 1 << i
            taken = (pltpu.roll(d, k, 0) == d) & (row >= k) & (group >= i)
            masks[i, :, :] = taken.astype(F32)
            count = count + jnp.where(taken, pltpu.roll(count, k, 0), 0.0)
        inv[...] = 1.0 / count

    step_rows = 16

    def normalize(l, c):
        def body(i, _):
            at_rows = pl.ds(pl.multiple_of(GATHER[l][c][0] + i * step_rows, step_rows), step_rows)
            total = jnp.zeros((step_rows, 1), F32)
            for b in range(TP):
                v = X[l, b, at_rows, :].astype(F32)
                total = total + jnp.sum(v * v, axis=-1, keepdims=True)
            r = lax.rsqrt(total * (1.0 / D) + EPS)
            for b in range(TP):
                v = X[l, b, at_rows, :].astype(F32)
                N[at_rows, pl.ds(b * width, width)] = (v * r * gain[pl.ds(l, 1), pl.ds(b * width, width)]).astype(BF16)
            return 0
        lax.fori_loop(0, GATHER[l][c][1] // step_rows, body, 0)

    def project(l, window):
        first, n = WINDOWS[l][window]
        w = W[l, :, pl.ds(0, depth_in), :].reshape(sps * depth_in, width)
        acc[pl.ds(0, n), :] = jnp.dot(N[pl.ds(first, n), :], w, preferred_element_type=F32)
        for cb in range(width // 128):
            cols = pl.ds(cb * 128, 128)
            p = acc[pl.ds(0, n), cols].astype(BF16).astype(F32)
            s = p
            for i in range(4):
                s = s + jnp.where(masks[i, pl.ds(first, n), :] > 0.5, pltpu.roll(s, 1 << i, 0), 0.0)
            pooled = (s * inv[pl.ds(first, n), :] - p).astype(BF16)
            G[l, half_of, pl.ds(first + 16, n - 16), cols] = pooled[16:, :]

    def mix(l, c):
        first, n = EXCHANGE[l][c]
        a = jnp.zeros((n, width), F32)
        for h in range(2):
            w = W[l, pl.ds(h * (sps // 2), sps // 2), pl.ds(depth_in, depth_mix), :].reshape(sps // 2 * depth_mix, width)
            a = a + jnp.dot(G[l, h, pl.ds(first, n), :], w, preferred_element_type=F32)
        a = a * scale[pl.ds(l, 1), pl.ds(pl.multiple_of(tp * width, width), width)]
        if l == 0:
            X[1, tp, pl.ds(first, n), :] = a.astype(BF16)
        else:
            out[pl.ds(first - HALO, n), :] = a.astype(BF16)

    halo_x = pltpu.make_async_remote_copy(X.at[0, tp, pl.ds(ext - HALO, HALO)], X.at[0, tp, pl.ds(0, HALO)], h_send.at[0], h_recv.at[0], device_id=(nxt, tp), device_id_type=MESH)
    halo_d = pltpu.make_async_remote_copy(docx.at[pl.ds(rows, HALO)], docx.at[pl.ds(0, HALO)], h_send.at[1], h_recv.at[1], device_id=(nxt, tp), device_id_type=MESH)
    halo_x.start()
    halo_d.start()

    def wait(token):
        name = token[0]
        if name == "w":
            layer, which = ROUNDS[token[1]]
            keys = GROUPS[token[1]][GROUP_OF[token[1]][token[2:]]]
            ref = W.at[layer, pl.ds(0, len(keys)), weight_rows[which]]
            if token[4] != "full":
                ref = ref.at[:, :, pl.ds(0, width // 2)]
            pltpu.make_async_copy(ref, ref, w_recv.at[FIRST[token[1]] + GROUP_OF[token[1]][token[2:]]]).wait()
            waited.update(("w", token[1]) + key for key in keys)
        elif name == "x":
            l, who, c = token[1:]
            x_copy(l, who, c, who, tp).wait_recv()
        elif name == "d":
            l, who, c = token[1:]
            d_copy(l, partner_block_of, who, c).wait_recv()
        elif name == "t":
            t_copy(*token[1:], tp).wait_recv()
        elif name == "e":
            l, c = token[1:]
            ref = G.at[l, 1 - half_of, span(EXCHANGE[l][c])]
            pltpu.make_async_remote_copy(ref, ref, e_send.at[l], e_recv.at[l, c], device_id=me, device_id_type=MESH).wait_recv()
        elif name == "halo":
            halo_x.wait_recv()
            halo_d.wait_recv()

    x_way = {1: x_plus, -1: x_minus}
    waited = set()
    ops, _, _ = build()
    for _, op, need in ops:
        for token in need:
            if token not in waited:
                waited.add(token)
                wait(token)
        name = op[0]
        if name == "ws":
            onward(*op[1:])
        elif name == "xs":
            l, who, c, way = op[1:]
            x_copy(l, who, c, {"o": "p" if way == 1 else "m"}.get(who, "2"), x_way[way]).start()
        elif name == "ds":
            d_copy(op[1], block_of, op[2], op[3]).start()
        elif name == "es":
            t_copy(*op[1:], x_way[1 if op[2] < 2 else -1]).start()
        elif name == "ed":
            l, c = op[1:]
            ref = G.at[l, half_of, span(EXCHANGE[l][c])]
            pltpu.make_async_remote_copy(ref, ref, e_send.at[l], e_recv.at[l, c], device_id=(sp, x_two), device_id_type=MESH).start()
        elif name == "ep":
            e_copy(*op[1:], x_way[1 if op[2] < 2 else -1]).start()
        elif name == "norm":
            normalize(op[1], op[2])
        elif name == "project":
            project(op[1], op[2])
        elif name == "mix":
            mix(op[1], op[2])
        elif name == "masks":
            make_masks()

    halo_x.wait_send()
    halo_d.wait_send()
    for r, (layer, which) in enumerate(ROUNDS):
        ref = W.at[layer, pl.ds(0, sps - 1), weight_rows[which]]
        pltpu.make_async_copy(ref, ref, w_send.at[r]).wait()
    for l in range(2):
        ref = X.at[l, pl.ds(0, 7), pl.ds(0, ext - l * HALO // 2)]
        pltpu.make_async_copy(ref, ref, x_send.at[l]).wait()
        ref = G.at[l, pl.ds(0, 1 if l in STRAIGHT else 2), pl.ds(0, ext - (l + 1) * HALO // 2)]
        pltpu.make_async_copy(ref, ref, e_send.at[l]).wait()


def shards(tokens, doc_ids, norm_gain, in_proj, mix_proj, out_scale):
    rows, width = tokens.shape
    depth_in, depth_mix = in_proj.shape[1], mix_proj.shape[1]
    ext = rows + HALO
    docs = doc_ids
    hbm = pl.BlockSpec(memory_space=pl.ANY)
    dma = pltpu.SemaphoreType.DMA
    return pl.pallas_call(
        functools.partial(kernel, rows, width, depth_in, depth_mix),
        name="mixer",
        out_shape=pltpu.VMEM((rows, width), BF16),
        in_specs=[hbm] * 6,
        out_specs=pl.BlockSpec(memory_space=pltpu.VMEM),
        scratch_shapes=[
            pltpu.VMEM((2, RING * RING, depth_in + depth_mix, width), BF16),
            pltpu.VMEM((2, TP, ext, width), BF16),
            pltpu.VMEM((ext, D), BF16),
            pltpu.VMEM((2, 2, ext, width), BF16),
            pltpu.VMEM((2, ext, width), BF16),
            pltpu.VMEM((ext, width), F32),
            pltpu.VMEM((ext, 128), F32),
            pltpu.VMEM((4, ext, 128), F32),
            pltpu.VMEM((ext, 128), F32),
            pltpu.VMEM((rows,), jnp.int32),
            pltpu.VMEM((2, D), F32),
            pltpu.VMEM((2, D), F32),
            dma((8,)),
            dma((len(ROUNDS),)),
            dma((FIRST[-1],)),
            dma((2,)),
            dma((2, 12)),
            dma((2, 16)),
            dma((2,)),
            dma((2, 4)),
            dma((2, 4)),
            dma((2,)),
            dma((2,)),
        ],
        compiler_params=pltpu.CompilerParams(collective_id=0, has_side_effects=True, vmem_limit_bytes=60 * 1024 * 1024),
    )(tokens, docs, norm_gain, in_proj, mix_proj, out_scale)


def solution(mesh):
    placed = (P("sp", "tp"), P("sp"), P(), P(None, "sp", "tp"), P(None, "sp", "tp"), P())
    return jax.shard_map(
        shards, mesh=mesh, in_specs=placed, out_specs=P("sp", "tp"), check_vma=False
    )
```

```python
import functools

import jax
import jax.numpy as jnp
from jax import lax
from jax.experimental import pallas as pl
from jax.experimental.pallas import tpu as pltpu
from jax.sharding import PartitionSpec as P

D = 4096
EPS = 1e-6
RING = 8
TP = 8
HALO = 32
MESH = pl.DeviceIdType.MESH
F32 = jnp.float32
BF16 = jnp.bfloat16

RATE, X_RATE, D_RATE = 92.0, 46.0, 560.0
HOP, X_HOP, D_HOP, DT = 2.8, 2.4, 1.6, 0.05
OFFS = (0, -1, 1, -2, 2, -3, 3, 4)
ROUNDS = ((0, 0), (0, 1), (1, 0), (1, 1))
BASE, STEP = (0, 2.6, 10, 13.6), (1, 1, 1, 1)
LIMIT = 0.55
STRAIGHT = (1,)
ROUTED = 0.75
LEAP = (3,)
PIECE_ROWS = (64, 16, 80)
SHARE = ((0, 1, 2, 3, 4), (0, 0, 0, 1, 1), (0, 1, 2, 3, 4), (0, 0, 0, 1, 1))
GATHER = (((0, 112), (112, 48), (160, 96), (256, 64)), ((16, 96), (112, 48), (160, 96), (256, 64)))
EXCHANGE = (GATHER[1], ((32, 80), (112, 64), (176, 80), (256, 64)))
WINDOWS = (((0, 320),), ((16, 96), (96, 80), (160, 96), (240, 80)))
WINDOW_OF = ((0, 0, 0, 0), (0, 1, 2, 3))
WINDOW_NEEDS = (((0, 1, 2, 3),), ((0,), (0, 1, 2), (2,), (2, 3)))
TIME = {"project": 2.3, "mix": 0.4, "norm": 0.7, "masks": 0.3, "halo": 0.1}
EARLY = {("norm", 0): 21.0}
SLACK = 3.0


LEAPS = [(0, way, far) for far in (2, 1) for way in (1, -1)] + [(-2 * way, way, far) for far in (2, 1) for way in (1, -1)]


def halves(last):
    return ("A", "B") if last == 4 else ("full",)


def message_groups():
    groups = []
    for r in range(len(ROUNDS)):
        members = {}
        for dl in OFFS:
            for dh in OFFS:
                for half in halves(dl if dh == 0 else dh) if (dl, dh) != (0, 0) else ():
                    name = (dl, 0, half) if dh == 0 else (SHARE[r][abs(dl)], dh, half, "h")
                    members.setdefault(name, []).append((dl, dh, half))
        groups.append(list(members.values()))
    return groups, [{key: i for i, keys in enumerate(g) for key in keys} for g in groups]


GROUPS, GROUP_OF = message_groups()


def build():
    rate = {"hF": RATE, "hB": RATE, "lF": RATE, "lB": RATE, "xF": X_RATE, "xB": X_RATE, "d": D_RATE}
    hops = {"x": X_HOP, "d": D_HOP}
    items, tasks = [], []

    def send(flow, kb, need, prio, gives, op):
        items.append([flow, kb, need, prio, gives, op])

    def task(need, op, gives, prio, time=None):
        tasks.append([need, time or TIME[op[0]], op, gives, prio])

    def all_pieces(layer, kind):
        return [("w", r, a, b, h) for r, round in enumerate(ROUNDS) if round[0] == layer and round[1] in (kind, 2)
                for a in OFFS for b in OFFS if (a, b) != (0, 0) for h in halves(a if b == 0 else b)]
    for r, (_, kind) in enumerate(ROUNDS):
        kb = PIECE_ROWS[kind] * 1.024
        for dl, (dh, way, far) in [(dl, leap) for dl in OFFS for leap in LEAPS] if r in LEAP else ():
            new = dh - way * far
            half = "full" if abs(new) < 4 else ("A" if way == 1 else "B")
            need = [("w", r, dl, dh, h) for h in halves(dl if dh == 0 else dh)] if (dl, dh) != (0, 0) else []
            send("hF" if way == 1 else "hB", kb * far / len(halves(abs(new))), need, (BASE[r] + (abs(dh) > 0) * STEP[r], -far, abs(dl)), ("w", r, dl, 4 if abs(new) == 4 else new, half), ("hl", r, dl, dh, way, far))
        for dl in OFFS:
            for dh in OFFS:
                for axis in ("l", "h") if dh == 0 else ("h",):
                    d = dl if axis == "l" else dh
                    if d == 4 or (axis == "h" and r in LEAP):
                        continue
                    for way in (1, -1) if d == 0 else ((1,) if d < 0 else (-1,)):
                        new, half = d - way, "full"
                        if abs(new) == 4:
                            new, half = 4, ("A" if way == 1 else "B")
                        key = (new, 0, half) if axis == "l" else (dl, new, half)
                        prio = (BASE[r] - 0.5, abs(dl)) if axis == "l" else (BASE[r] + abs(d) * STEP[r], abs(dl))
                        need = [] if (dl, dh) == (0, 0) else [("w", r, dl, dh, h) for h in halves(dl if dh == 0 else dh)]
                        send(axis + ("F" if way == 1 else "B"), kb / len(halves(new)), need, prio, ("w", r) + key, ("ws", r, dl, dh, axis, way))
    for l in range(2):
        for c in range(4):
            own, kb, phase, side = [("cur", l, c)], GATHER[l][c][1] * 1.024, c % 2, c // 2
            send("xF", kb, own, (l, 0, phase, side), ("x", l, "p", c), ("xs", l, "o", c, 1))
            send("xB", kb, own, (l, 0, phase, 1 - side), ("x", l, "m", c), ("xs", l, "o", c, -1))
            send("d", kb, own, (l, 0, c), ("d", l, "o", c), ("ds", l, "o", c))
            way = 1 - 2 * side
            send(("xF", "xB")[side], kb, [("x", l, "pm"[side], c)], (l, 0, phase, -1), ("x", l, "2", c), ("xs", l, "pm"[side], c, way))
            for who in ("p", "m", "2"):
                send("d", kb, [("x", l, who, c)], (l, 1, c), ("d", l, who, c), ("ds", l, who, c))
            need = [("x", l, w, c) for w in ("p", "m", "2")] + [("d", l, w, c) for w in ("o", "p", "m", "2")] + own
            task(need, ("norm", l, c), [("n", l, c)], (l, 0, phase, c))
            kb = EXCHANGE[l][c][1] * 1.024
            if l in STRAIGHT:
                send(("xF", "xB")[side], 2 * kb, [("pool", l, WINDOW_OF[l][c])], (l, 1, phase, 0), ("e", l, c), ("ed", l, c))
            else:
                send(("xF", "xB")[side], kb, [("pool", l, WINDOW_OF[l][c])], (l, 1, phase, 0), ("t", l, c), ("es", l, c))
                send(("xF", "xB")[side], kb, [("t", l, c)], (l, 1, phase, -1), ("e", l, c), ("ep", l, c))
            task([("e", l, c), ("pool", l, WINDOW_OF[l][c])] + all_pieces(l, 1), ("mix", l, c), [("cur", l + 1, c)], (l, 2, phase, c))
        for w, needs in enumerate(WINDOW_NEEDS[l]):
            task(all_pieces(l, 0) + [("n", l, c) for c in needs] + [("masks",)], ("project", l, w), [("pool", l, w)], (l, 1, w % 2, w), (2.3, 1.0)[l])
    task([("halo",)], ("halo",), [("cur", 0, 0)], (-1, 0, 0, 0))
    task([("halo",)], ("masks",), [("masks",)], (0, -1, 0, 0))
    have = {("cur", 0, c): 0.0 for c in range(1, 4)}
    arrivals, finishing, landed = [(7.0, ("halo",))], [], {}
    flows = {f: [] for f in rate}
    ops, t, busy, done_at = [], 0.0, 0.0, {}
    items.sort(key=lambda i: i[3])
    tasks.sort(key=lambda k: k[4])
    while items or tasks:
        for a in [a for a in arrivals if a[0] <= t + 1e-9]:
            arrivals.remove(a)
            if a[1][0] == "w":
                r, group = a[1][1], (a[1][1], GROUP_OF[a[1][1]][a[1][2:]])
                landed[group] = landed.get(group, 0) + 1
                if landed[group] == len(GROUPS[r][group[1]]):
                    have.update({("w", r) + key: a[0] for key in GROUPS[r][group[1]]})
            else:
                have[a[1]] = a[0]
        for a in [a for a in finishing if a[0] <= t + 1e-9]:
            finishing.remove(a)
            for g in a[1]:
                have[g] = t
        if t >= busy - 1e-9:
            again = True
            while again:
                again = False
                for i in items:
                    f = i[0]
                    if sum(x[1] for x in flows[f]) / rate[f] <= LIMIT and all(n in have for n in i[2]):
                        items.remove(i)
                        flows[f].append([i, i[1]])
                        ops.append((t, i[5], i[2]))
                        again = True
                        break
            for k in tasks:
                if t >= EARLY.get(k[2][:2], 0.0) and all(n in have for n in k[0]):
                    tasks.remove(k)
                    ops.append((t, k[2], k[0]))
                    busy = t + k[1]
                    finishing.append((busy, k[3]))
                    done_at[k[2]] = busy
                    break
        active = {f: bool(flows[f]) for f in flows}
        for f in flows:
            share = 1.0 / (active["h" + f[1]] + active["l" + f[1]]) if active[f] and f[0] in "hl" else 1.0
            left = rate[f] * share * DT
            while flows[f] and left > 0:
                q = flows[f][0]
                use = min(left, q[1])
                q[1] -= use
                left -= use
                if q[1] <= 1e-9:
                    flows[f].pop(0)
                    arrivals.append((t + DT + hops.get(f[0], HOP) + (SLACK if q[0][4][0] in ("x", "d") and q[0][4][1] == 0 else 0.0) + (ROUTED if q[0][5][0] == "ed" or q[0][5][-1] == 2 and q[0][5][0] == "hl" else 0.0), q[0][4]))
        t += DT
    return ops, done_at, have


FIRST = [sum(len(g) for g in GROUPS[:r]) for r in range(len(ROUNDS) + 1)]
WHO = {"p": 0, "m": 1, "2": 2, "o": 3}


def kernel(rows, width, depth_in, depth_mix,
           tok, docs_in, gain_in, w_in, w_mix, scale_in, out,
           W, X, N, G, T, acc, docx, masks, inv, docs, gain, scale,
           load_sem, w_send, w_recv, x_send, x_recv, d_recv, e_send, t_recv, e_recv, h_send, h_recv):
    ext = rows + HALO
    sp, tp = lax.axis_index("sp"), lax.axis_index("tp")
    core = lax.rem(tp, 2)
    z, y = sp // RING, lax.rem(sp, RING)
    sps = RING * RING

    def at(dl, dh):
        ay = dl + core * (dh - dl)
        az = dh + core * (dl - dh)
        return lax.rem(z + az + RING, RING) * RING + lax.rem(y + ay + RING, RING)

    partner = tp + 1 - 2 * core
    x_plus, x_minus, x_two = lax.rem(tp + 2, TP), lax.rem(tp + TP - 2, TP), lax.rem(tp + 4, TP)
    nxt, prv = lax.rem(sp + 1, sps), lax.rem(sp + sps - 1, sps)
    target = {("l", 1): at(1, 0), ("l", -1): at(-1, 0), ("h", 1): at(0, 1), ("h", -1): at(0, -1)}
    me = (sp, tp)

    barrier = pltpu.get_barrier_semaphore()
    neighbours = [(d, tp) for d in target.values()] + [(nxt, tp), (prv, tp), (sp, x_plus), (sp, x_minus), (sp, x_two), (sp, partner), (at(0, 2), tp), (at(0, -2), tp)]
    for n in neighbours:
        pl.semaphore_signal(barrier, inc=1, device_id=n, device_id_type=MESH)

    def spread_docs():
        for k in range(0, rows, 128):
            n = min(128, rows - k)
            line = docs[pl.ds(k, n)].astype(F32).reshape(1, n)
            if n < 128:
                line = jnp.concatenate([line, jnp.zeros((1, 128 - n), F32)], axis=1)
            docx[pl.ds(HALO + k, n), :] = jnp.transpose(jnp.broadcast_to(line, (128, 128)))[:n, :]

    weight_rows = (pl.ds(0, depth_in), pl.ds(depth_in, depth_mix), pl.ds(0, depth_in + depth_mix))
    small = [pltpu.make_async_copy(docs_in, docs, load_sem.at[5]), pltpu.make_async_copy(gain_in, gain, load_sem.at[6]), pltpu.make_async_copy(scale_in, scale, load_sem.at[7])]
    loads = [pltpu.make_async_copy(tok, X.at[0, tp, pl.ds(HALO, rows)], load_sem.at[4])]
    for layer in range(2):
        for is_mix in range(2):
            loads.append(pltpu.make_async_copy((w_in, w_mix)[is_mix].at[layer], W.at[layer, sp, weight_rows[is_mix]], load_sem.at[2 * layer + is_mix]))
    for c in small[:1] + loads + small[1:]:
        c.start()
    small[0].wait()
    spread_docs()
    for c in loads + small[1:]:
        c.wait()
    pl.semaphore_wait(barrier, len(neighbours))

    def w_copy(r, dl, dh, half, key, device):
        layer, which = ROUNDS[r]
        ref = W.at[layer, at(dl, dh), weight_rows[which]]
        if half != "full":
            ref = ref.at[:, pl.ds(0 if half == "A" else width // 2, width // 2)]
        return pltpu.make_async_remote_copy(ref, ref, w_send.at[r], w_recv.at[FIRST[r] + GROUP_OF[r][key]], device_id=(device, tp), device_id_type=MESH)

    def onward(r, dl, dh, axis, way):
        new, half = (dl if axis == "l" else dh) - way, "full"
        if abs(new) == 4:
            new, half = 4, ("A" if way == 1 else "B")
        key = (new, 0, half) if axis == "l" else (dl, new, half)
        w_copy(r, dl, dh, half, key, target[axis, way]).start()

    def span(chunk):
        return pl.ds(*chunk)

    def blocks(first):
        return {"o": first, "p": lax.rem(first + TP - 2, TP), "m": lax.rem(first + 2, TP), "2": lax.rem(first + 4, TP)}

    block_of = blocks(tp)

    def x_copy(l, who, c, key, device):
        ref = X.at[l, block_of[who], span(GATHER[l][c])]
        return pltpu.make_async_remote_copy(ref, ref, x_send.at[l], x_recv.at[l, WHO[key] * 4 + c], device_id=(sp, device), device_id_type=MESH)

    def d_copy(l, who, c):
        ref = X.at[l, block_of[who], span(GATHER[l][c])]
        return pltpu.make_async_remote_copy(ref, ref, x_send.at[l], d_recv.at[l, c], device_id=(sp, partner), device_id_type=MESH)

    half_of = tp // (TP // 2)

    def t_copy(l, c, device):
        rows_of = span(EXCHANGE[l][c])
        return pltpu.make_async_remote_copy(G.at[l, half_of, rows_of], T.at[l, rows_of], e_send.at[l], t_recv.at[l, c], device_id=(sp, device), device_id_type=MESH)

    def e_copy(l, c, device):
        rows_of, slot = span(EXCHANGE[l][c]), 1 - device // (TP // 2)
        return pltpu.make_async_remote_copy(T.at[l, rows_of], G.at[l, slot, rows_of], e_send.at[l], e_recv.at[l, c], device_id=(sp, device), device_id_type=MESH)

    def make_masks():
        docx[pl.ds(0, HALO), :] = jnp.where(sp == 0, jnp.float32(-1.0), docx[pl.ds(0, HALO), :])
        d = docx[...]
        row = lax.broadcasted_iota(jnp.int32, (ext, 128), 0)
        group = lax.rem(tp, 4)
        count = jnp.ones((ext, 128), F32)
        for i in range(4):
            k = 1 << i
            taken = (pltpu.roll(d, k, 0) == d) & (row >= k) & (group >= i)
            masks[i, :, :] = taken.astype(F32)
            count = count + jnp.where(taken, pltpu.roll(count, k, 0), 0.0)
        inv[...] = 1.0 / count

    step_rows = 16

    def normalize(l, c):
        def body(i, _):
            at_rows = pl.ds(pl.multiple_of(GATHER[l][c][0] + i * step_rows, step_rows), step_rows)
            total = jnp.zeros((step_rows, 1), F32)
            for b in range(TP):
                v = X[l, b, at_rows, :].astype(F32)
                total = total + jnp.sum(v * v, axis=-1, keepdims=True)
            r = lax.rsqrt(total * (1.0 / D) + EPS)
            for b in range(TP):
                v = X[l, b, at_rows, :].astype(F32)
                N[at_rows, pl.ds(b * width, width)] = (v * r * gain[pl.ds(l, 1), pl.ds(b * width, width)]).astype(BF16)
            return 0
        lax.fori_loop(0, GATHER[l][c][1] // step_rows, body, 0)

    def project(l, window):
        first, n = WINDOWS[l][window]
        w = W[l, :, pl.ds(0, depth_in), :].reshape(sps * depth_in, width)
        acc[pl.ds(0, n), :] = jnp.dot(N[pl.ds(first, n), :], w, preferred_element_type=F32)
        for cb in range(width // 128):
            cols = pl.ds(cb * 128, 128)
            p = acc[pl.ds(0, n), cols].astype(BF16).astype(F32)
            s = p
            for i in range(4):
                s = s + jnp.where(masks[i, pl.ds(first, n), :] > 0.5, pltpu.roll(s, 1 << i, 0), 0.0)
            pooled = (s * inv[pl.ds(first, n), :] - p).astype(BF16)
            G[l, half_of, pl.ds(first + 16, n - 16), cols] = pooled[16:, :]

    def mix(l, c):
        first, n = EXCHANGE[l][c]
        a = jnp.zeros((n, width), F32)
        for h in range(2):
            w = W[l, pl.ds(h * (sps // 2), sps // 2), pl.ds(depth_in, depth_mix), :].reshape(sps // 2 * depth_mix, width)
            a = a + jnp.dot(G[l, h, pl.ds(first, n), :], w, preferred_element_type=F32)
        a = a * scale[pl.ds(l, 1), pl.ds(pl.multiple_of(tp * width, width), width)]
        if l == 0:
            X[1, tp, pl.ds(first, n), :] = a.astype(BF16)
        else:
            out[pl.ds(first - HALO, n), :] = a.astype(BF16)

    halo_x = pltpu.make_async_remote_copy(X.at[0, tp, pl.ds(ext - HALO, HALO)], X.at[0, tp, pl.ds(0, HALO)], h_send.at[0], h_recv.at[0], device_id=(nxt, tp), device_id_type=MESH)
    halo_d = pltpu.make_async_remote_copy(docx.at[pl.ds(rows, HALO)], docx.at[pl.ds(0, HALO)], h_send.at[1], h_recv.at[1], device_id=(nxt, tp), device_id_type=MESH)
    halo_x.start()
    halo_d.start()

    def wait(token):
        name = token[0]
        if name == "w":
            layer, which = ROUNDS[token[1]]
            keys = GROUPS[token[1]][GROUP_OF[token[1]][token[2:]]]
            ref = W.at[layer, pl.ds(0, len(keys)), weight_rows[which]]
            if token[4] != "full":
                ref = ref.at[:, :, pl.ds(0, width // 2)]
            pltpu.make_async_copy(ref, ref, w_recv.at[FIRST[token[1]] + GROUP_OF[token[1]][token[2:]]]).wait()
            waited.update(("w", token[1]) + key for key in keys)
        elif name == "x":
            l, who, c = token[1:]
            x_copy(l, who, c, who, tp).wait_recv()
        elif name == "d":
            l, _, c = token[1:]
            ref = X.at[l, pl.ds(0, 4), span(GATHER[l][c])]
            pltpu.make_async_copy(ref, ref, d_recv.at[l, c]).wait()
            waited.update(("d", l, who, c) for who in WHO)
        elif name == "t":
            t_copy(*token[1:], tp).wait_recv()
        elif name == "e":
            l, c = token[1:]
            ref = G.at[l, 1 - half_of, span(EXCHANGE[l][c])]
            pltpu.make_async_remote_copy(ref, ref, e_send.at[l], e_recv.at[l, c], device_id=me, device_id_type=MESH).wait_recv()
        elif name == "halo":
            halo_x.wait_recv()
            halo_d.wait_recv()

    x_way = {1: x_plus, -1: x_minus}
    waited = set()
    ops, _, _ = build()
    for _, op, need in ops:
        for token in need:
            if token not in waited:
                waited.add(token)
                wait(token)
        name = op[0]
        if name == "ws":
            onward(*op[1:])
        elif name == "xs":
            l, who, c, way = op[1:]
            x_copy(l, who, c, {"o": "p" if way == 1 else "m"}.get(who, "2"), x_way[way]).start()
        elif name == "ds":
            d_copy(*op[1:]).start()
        elif name == "es":
            t_copy(*op[1:], x_way[1 if op[2] < 2 else -1]).start()
        elif name == "hl":
            r, dl, dh, way, far = op[1:]
            new = dh - way * far
            half = "full" if abs(new) < 4 else ("A" if way == 1 else "B")
            w_copy(r, dl, dh, half, (dl, 4 if abs(new) == 4 else new, half), at(0, way * far)).start()
        elif name == "ed":
            l, c = op[1:]
            ref = G.at[l, half_of, span(EXCHANGE[l][c])]
            pltpu.make_async_remote_copy(ref, ref, e_send.at[l], e_recv.at[l, c], device_id=(sp, x_two), device_id_type=MESH).start()
        elif name == "ep":
            e_copy(*op[1:], x_way[1 if op[2] < 2 else -1]).start()
        elif name == "norm":
            normalize(op[1], op[2])
        elif name == "project":
            project(op[1], op[2])
        elif name == "mix":
            mix(op[1], op[2])
        elif name == "masks":
            make_masks()

    halo_x.wait_send()
    halo_d.wait_send()
    for r, (layer, which) in enumerate(ROUNDS):
        ref = W.at[layer, pl.ds(0, sps - 1), weight_rows[which]]
        pltpu.make_async_copy(ref, ref, w_send.at[r]).wait()
    for l in range(2):
        ref = X.at[l, pl.ds(0, 7), pl.ds(0, ext - l * HALO // 2)]
        pltpu.make_async_copy(ref, ref, x_send.at[l]).wait()
        ref = G.at[l, pl.ds(0, 1 if l in STRAIGHT else 2), pl.ds(0, ext - (l + 1) * HALO // 2)]
        pltpu.make_async_copy(ref, ref, e_send.at[l]).wait()


def shards(tokens, doc_ids, norm_gain, in_proj, mix_proj, out_scale):
    rows, width = tokens.shape
    depth_in, depth_mix = in_proj.shape[1], mix_proj.shape[1]
    ext = rows + HALO
    docs = doc_ids
    hbm = pl.BlockSpec(memory_space=pl.ANY)
    dma = pltpu.SemaphoreType.DMA
    return pl.pallas_call(
        functools.partial(kernel, rows, width, depth_in, depth_mix),
        name="mixer",
        out_shape=pltpu.VMEM((rows, width), BF16),
        in_specs=[hbm] * 6,
        out_specs=pl.BlockSpec(memory_space=pltpu.VMEM),
        scratch_shapes=[
            pltpu.VMEM((2, RING * RING, depth_in + depth_mix, width), BF16),
            pltpu.VMEM((2, TP, ext, width), BF16),
            pltpu.VMEM((ext, D), BF16),
            pltpu.VMEM((2, 2, ext, width), BF16),
            pltpu.VMEM((2, ext, width), BF16),
            pltpu.VMEM((ext, width), F32),
            pltpu.VMEM((ext, 128), F32),
            pltpu.VMEM((4, ext, 128), F32),
            pltpu.VMEM((ext, 128), F32),
            pltpu.VMEM((rows,), jnp.int32),
            pltpu.VMEM((2, D), F32),
            pltpu.VMEM((2, D), F32),
            dma((8,)),
            dma((len(ROUNDS),)),
            dma((FIRST[-1],)),
            dma((2,)),
            dma((2, 12)),
            dma((2, 4)),
            dma((2,)),
            dma((2, 4)),
            dma((2, 4)),
            dma((2,)),
            dma((2,)),
        ],
        compiler_params=pltpu.CompilerParams(collective_id=0, has_side_effects=True, vmem_limit_bytes=60 * 1024 * 1024),
    )(tokens, docs, norm_gain, in_proj, mix_proj, out_scale)


def solution(mesh):
    placed = (P("sp", "tp"), P("sp"), P(), P(None, "sp", "tp"), P(None, "sp", "tp"), P())
    return jax.shard_map(
        shards, mesh=mesh, in_specs=placed, out_specs=P("sp", "tp"), check_vma=False
    )
```

```python
import functools

import jax
import jax.numpy as jnp
from jax import lax
from jax.experimental import pallas as pl
from jax.experimental.pallas import tpu as pltpu
from jax.sharding import PartitionSpec as P

D = 4096
EPS = 1e-6
RING = 8
TP = 8
HALO = 32
MESH = pl.DeviceIdType.MESH
F32 = jnp.float32
BF16 = jnp.bfloat16

RATE, X_RATE, D_RATE = 89.0, 44.5, 500.0
HOP, X_HOP, D_HOP, DT = 2.8, 2.4, 1.6, 0.05
OFFS = (0, -1, 1, -2, 2, -3, 3, 4)
ROUNDS = ((0, 0), (0, 1), (1, 0), (1, 1))
BASE, STEP = (0, 2.6, 10, 13.6), (1, 1, 1, 1)
LIMIT = 0.55
STRAIGHT = (1,)
ROUTED = 0.75
LEAP = (3,)
PIECE_ROWS = (64, 16, 80)
SHARE = ((0, 1, 2, 3, 4), (0, 0, 0, 1, 1), (0, 1, 2, 3, 4), (0, 0, 0, 1, 1))
GATHER = (((0, 112), (112, 48), (160, 96), (256, 64)), ((16, 96), (112, 48), (160, 96), (256, 64)))
EXCHANGE = (GATHER[1], ((32, 80), (112, 64), (176, 80), (256, 64)))
WINDOWS = (((0, 320),), ((16, 96), (96, 80), (160, 96), (240, 80)))
WINDOW_OF = ((0, 0, 0, 0), (0, 1, 2, 3))
WINDOW_NEEDS = (((0, 1, 2, 3),), ((0,), (0, 1, 2), (2,), (2, 3)))
TIME = {"project": 2.3, "mix": 0.4, "norm": 0.7, "masks": 0.3, "halo": 0.1}
EARLY = {("norm", 0): 21.0}
SLACK = 3.0


LEAPS = [(0, way, far) for far in (2, 1) for way in (1, -1)] + [(-2 * way, way, far) for far in (2, 1) for way in (1, -1)]


def halves(last):
    return ("A", "B") if last == 4 else ("full",)


def message_groups():
    groups = []
    for r in range(len(ROUNDS)):
        members = {}
        for dl in OFFS:
            for dh in OFFS:
                for half in halves(dl if dh == 0 else dh) if (dl, dh) != (0, 0) else ():
                    name = (dl, 0, half) if dh == 0 else (SHARE[r][abs(dl)], dh, half, "h")
                    members.setdefault(name, []).append((dl, dh, half))
        groups.append(list(members.values()))
    return groups, [{key: i for i, keys in enumerate(g) for key in keys} for g in groups]


GROUPS, GROUP_OF = message_groups()


def build():
    rate = {"hF": RATE, "hB": RATE, "lF": RATE, "lB": RATE, "xF": X_RATE, "xB": X_RATE, "d": D_RATE}
    hops = {"x": X_HOP, "d": D_HOP}
    items, tasks = [], []

    def send(flow, kb, need, prio, gives, op):
        items.append([flow, kb, need, prio, gives, op])

    def task(need, op, gives, prio, time=None):
        tasks.append([need, time or TIME[op[0]], op, gives, prio])

    def all_pieces(layer, kind):
        return [("w", r, a, b, h) for r, round in enumerate(ROUNDS) if round[0] == layer and round[1] in (kind, 2)
                for a in OFFS for b in OFFS if (a, b) != (0, 0) for h in halves(a if b == 0 else b)]
    for r, (_, kind) in enumerate(ROUNDS):
        kb = PIECE_ROWS[kind] * 1.024
        for dl, (dh, way, far) in [(dl, leap) for dl in OFFS for leap in LEAPS] if r in LEAP else ():
            new = dh - way * far
            half = "full" if abs(new) < 4 else ("A" if way == 1 else "B")
            need = [("w", r, dl, dh, h) for h in halves(dl if dh == 0 else dh)] if (dl, dh) != (0, 0) else []
            send("hF" if way == 1 else "hB", kb * far / len(halves(abs(new))), need, (BASE[r] + (abs(dh) > 0) * STEP[r], -far, abs(dl)), ("w", r, dl, 4 if abs(new) == 4 else new, half), ("hl", r, dl, dh, way, far))
        for dl in OFFS:
            for dh in OFFS:
                for axis in ("l", "h") if dh == 0 else ("h",):
                    d = dl if axis == "l" else dh
                    if d == 4 or (axis == "h" and r in LEAP):
                        continue
                    for way in (1, -1) if d == 0 else ((1,) if d < 0 else (-1,)):
                        new, half = d - way, "full"
                        if abs(new) == 4:
                            new, half = 4, ("A" if way == 1 else "B")
                        key = (new, 0, half) if axis == "l" else (dl, new, half)
                        prio = (BASE[r] - 0.5, abs(dl)) if axis == "l" else (BASE[r] + abs(d) * STEP[r], abs(dl))
                        need = [] if (dl, dh) == (0, 0) else [("w", r, dl, dh, h) for h in halves(dl if dh == 0 else dh)]
                        send(axis + ("F" if way == 1 else "B"), kb / len(halves(new)), need, prio, ("w", r) + key, ("ws", r, dl, dh, axis, way))
    for l in range(2):
        for c in range(4):
            own, kb, phase, side = [("cur", l, c)], GATHER[l][c][1] * 1.024, c % 2, c // 2
            send("xF", kb, own, (l, 0, phase, side), ("x", l, "p", c), ("xs", l, "o", c, 1))
            send("xB", kb, own, (l, 0, phase, 1 - side), ("x", l, "m", c), ("xs", l, "o", c, -1))
            send("d", kb, own, (l, 0, c), ("d", l, "o", c), ("ds", l, "o", c))
            way = 1 - 2 * side
            send(("xF", "xB")[side], kb, [("x", l, "pm"[side], c)], (l, 0, phase, -1), ("x", l, "2", c), ("xs", l, "pm"[side], c, way))
            for who in ("p", "m", "2"):
                send("d", kb, [("x", l, who, c)], (l, 1, c), ("d", l, who, c), ("ds", l, who, c))
            need = [("x", l, w, c) for w in ("p", "m", "2")] + [("d", l, w, c) for w in ("o", "p", "m", "2")] + own
            task(need, ("norm", l, c), [("n", l, c)], (l, 0, phase, c))
            kb = EXCHANGE[l][c][1] * 1.024
            if l in STRAIGHT:
                send(("xF", "xB")[side], 2 * kb, [("pool", l, WINDOW_OF[l][c])], (l, 1, phase, 0), ("e", l, c), ("ed", l, c))
            else:
                send(("xF", "xB")[side], kb, [("pool", l, WINDOW_OF[l][c])], (l, 1, phase, 0), ("t", l, c), ("es", l, c))
                send(("xF", "xB")[side], kb, [("t", l, c)], (l, 1, phase, -1), ("e", l, c), ("ep", l, c))
            task([("e", l, c), ("pool", l, WINDOW_OF[l][c])] + all_pieces(l, 1), ("mix", l, c), [("cur", l + 1, c)], (l, 2, phase, c))
        for w, needs in enumerate(WINDOW_NEEDS[l]):
            task(all_pieces(l, 0) + [("n", l, c) for c in needs] + [("masks",)], ("project", l, w), [("pool", l, w)], (l, 1, w % 2, w), (2.3, 1.0)[l])
    task([("halo",)], ("halo",), [("cur", 0, 0)], (-1, 0, 0, 0))
    task([("halo",)], ("masks",), [("masks",)], (0, -1, 0, 0))
    have = {("cur", 0, c): 0.0 for c in range(1, 4)}
    arrivals, finishing, landed = [(7.0, ("halo",))], [], {}
    flows = {f: [] for f in rate}
    ops, t, busy, done_at = [], 0.0, 0.0, {}
    items.sort(key=lambda i: i[3])
    tasks.sort(key=lambda k: k[4])
    while items or tasks:
        for a in [a for a in arrivals if a[0] <= t + 1e-9]:
            arrivals.remove(a)
            if a[1][0] == "w":
                r, group = a[1][1], (a[1][1], GROUP_OF[a[1][1]][a[1][2:]])
                landed[group] = landed.get(group, 0) + 1
                if landed[group] == len(GROUPS[r][group[1]]):
                    have.update({("w", r) + key: a[0] for key in GROUPS[r][group[1]]})
            else:
                have[a[1]] = a[0]
        for a in [a for a in finishing if a[0] <= t + 1e-9]:
            finishing.remove(a)
            for g in a[1]:
                have[g] = t
        if t >= busy - 1e-9:
            again = True
            while again:
                again = False
                for i in items:
                    f = i[0]
                    if sum(x[1] for x in flows[f]) / rate[f] <= LIMIT and all(n in have for n in i[2]):
                        items.remove(i)
                        flows[f].append([i, i[1]])
                        ops.append((t, i[5], i[2]))
                        again = True
                        break
            for k in tasks:
                if t >= EARLY.get(k[2][:2], 0.0) and all(n in have for n in k[0]):
                    tasks.remove(k)
                    ops.append((t, k[2], k[0]))
                    busy = t + k[1]
                    finishing.append((busy, k[3]))
                    done_at[k[2]] = busy
                    break
        active = {f: bool(flows[f]) for f in flows}
        for f in flows:
            share = 1.0 / (active["h" + f[1]] + active["l" + f[1]]) if active[f] and f[0] in "hl" else 1.0
            left = rate[f] * share * DT
            while flows[f] and left > 0:
                q = flows[f][0]
                use = min(left, q[1])
                q[1] -= use
                left -= use
                if q[1] <= 1e-9:
                    flows[f].pop(0)
                    arrivals.append((t + DT + hops.get(f[0], HOP) + (SLACK if q[0][4][0] in ("x", "d") and q[0][4][1] == 0 else 0.0) + (ROUTED if q[0][5][0] == "ed" or q[0][5][-1] == 2 and q[0][5][0] == "hl" else 0.0), q[0][4]))
        t += DT
    return ops, done_at, have


FIRST = [sum(len(g) for g in GROUPS[:r]) for r in range(len(ROUNDS) + 1)]
WHO = {"p": 0, "m": 1, "2": 2, "o": 3}


def kernel(rows, width, depth_in, depth_mix,
           tok, docs_in, gain_in, w_in, w_mix, scale_in, out,
           W, X, N, G, T, acc, docx, masks, inv, docs, gain, scale,
           load_sem, w_send, w_recv, x_send, x_recv, d_recv, e_send, t_recv, e_recv, h_send, h_recv):
    ext = rows + HALO
    sp, tp = lax.axis_index("sp"), lax.axis_index("tp")
    core = lax.rem(tp, 2)
    z, y = sp // RING, lax.rem(sp, RING)
    sps = RING * RING

    def at(dl, dh):
        ay = dl + core * (dh - dl)
        az = dh + core * (dl - dh)
        return lax.rem(z + az + RING, RING) * RING + lax.rem(y + ay + RING, RING)

    partner = tp + 1 - 2 * core
    x_plus, x_minus, x_two = lax.rem(tp + 2, TP), lax.rem(tp + TP - 2, TP), lax.rem(tp + 4, TP)
    nxt, prv = lax.rem(sp + 1, sps), lax.rem(sp + sps - 1, sps)
    target = {("l", 1): at(1, 0), ("l", -1): at(-1, 0), ("h", 1): at(0, 1), ("h", -1): at(0, -1)}
    me = (sp, tp)

    barrier = pltpu.get_barrier_semaphore()
    neighbours = [(d, tp) for d in target.values()] + [(nxt, tp), (prv, tp), (sp, x_plus), (sp, x_minus), (sp, x_two), (sp, partner), (at(0, 2), tp), (at(0, -2), tp)]
    for n in neighbours:
        pl.semaphore_signal(barrier, inc=1, device_id=n, device_id_type=MESH)

    def spread_docs():
        for k in range(0, rows, 128):
            n = min(128, rows - k)
            line = docs[pl.ds(k, n)].astype(F32).reshape(1, n)
            if n < 128:
                line = jnp.concatenate([line, jnp.zeros((1, 128 - n), F32)], axis=1)
            docx[pl.ds(HALO + k, n), :] = jnp.transpose(jnp.broadcast_to(line, (128, 128)))[:n, :]

    weight_rows = (pl.ds(0, depth_in), pl.ds(depth_in, depth_mix), pl.ds(0, depth_in + depth_mix))
    small = [pltpu.make_async_copy(docs_in, docs, load_sem.at[5]), pltpu.make_async_copy(gain_in, gain, load_sem.at[6]), pltpu.make_async_copy(scale_in, scale, load_sem.at[7])]
    loads = [pltpu.make_async_copy(tok, X.at[0, tp, pl.ds(HALO, rows)], load_sem.at[4])]
    for layer in range(2):
        for is_mix in range(2):
            loads.append(pltpu.make_async_copy((w_in, w_mix)[is_mix].at[layer], W.at[layer, sp, weight_rows[is_mix]], load_sem.at[2 * layer + is_mix]))
    for c in small[:1] + loads + small[1:]:
        c.start()
    small[0].wait()
    spread_docs()
    for c in loads + small[1:]:
        c.wait()
    pl.semaphore_wait(barrier, len(neighbours))

    def w_copy(r, dl, dh, half, key, device):
        layer, which = ROUNDS[r]
        ref = W.at[layer, at(dl, dh), weight_rows[which]]
        if half != "full":
            ref = ref.at[:, pl.ds(0 if half == "A" else width // 2, width // 2)]
        return pltpu.make_async_remote_copy(ref, ref, w_send.at[r], w_recv.at[FIRST[r] + GROUP_OF[r][key]], device_id=(device, tp), device_id_type=MESH)

    def onward(r, dl, dh, axis, way):
        new, half = (dl if axis == "l" else dh) - way, "full"
        if abs(new) == 4:
            new, half = 4, ("A" if way == 1 else "B")
        key = (new, 0, half) if axis == "l" else (dl, new, half)
        w_copy(r, dl, dh, half, key, target[axis, way]).start()

    def span(chunk):
        return pl.ds(*chunk)

    def blocks(first):
        return {"o": first, "p": lax.rem(first + TP - 2, TP), "m": lax.rem(first + 2, TP), "2": lax.rem(first + 4, TP)}

    block_of = blocks(tp)

    def x_copy(l, who, c, key, device):
        ref = X.at[l, block_of[who], span(GATHER[l][c])]
        return pltpu.make_async_remote_copy(ref, ref, x_send.at[l], x_recv.at[l, WHO[key] * 4 + c], device_id=(sp, device), device_id_type=MESH)

    def d_copy(l, who, c):
        ref = X.at[l, block_of[who], span(GATHER[l][c])]
        return pltpu.make_async_remote_copy(ref, ref, x_send.at[l], d_recv.at[l, c], device_id=(sp, partner), device_id_type=MESH)

    half_of = tp // (TP // 2)

    def t_copy(l, c, device):
        rows_of = span(EXCHANGE[l][c])
        return pltpu.make_async_remote_copy(G.at[l, half_of, rows_of], T.at[l, rows_of], e_send.at[l], t_recv.at[l, c], device_id=(sp, device), device_id_type=MESH)

    def e_copy(l, c, device):
        rows_of, slot = span(EXCHANGE[l][c]), 1 - device // (TP // 2)
        return pltpu.make_async_remote_copy(T.at[l, rows_of], G.at[l, slot, rows_of], e_send.at[l], e_recv.at[l, c], device_id=(sp, device), device_id_type=MESH)

    def make_masks():
        docx[pl.ds(0, HALO), :] = jnp.where(sp == 0, jnp.float32(-1.0), docx[pl.ds(0, HALO), :])
        d = docx[...]
        row = lax.broadcasted_iota(jnp.int32, (ext, 128), 0)
        group = lax.rem(tp, 4)
        count = jnp.ones((ext, 128), F32)
        for i in range(4):
            k = 1 << i
            taken = (pltpu.roll(d, k, 0) == d) & (row >= k) & (group >= i)
            masks[i, :, :] = taken.astype(F32)
            count = count + jnp.where(taken, pltpu.roll(count, k, 0), 0.0)
        inv[...] = 1.0 / count

    step_rows = 16

    def normalize(l, c):
        def body(i, _):
            at_rows = pl.ds(pl.multiple_of(GATHER[l][c][0] + i * step_rows, step_rows), step_rows)
            total = jnp.zeros((step_rows, 1), F32)
            for b in range(TP):
                v = X[l, b, at_rows, :].astype(F32)
                total = total + jnp.sum(v * v, axis=-1, keepdims=True)
            r = lax.rsqrt(total * (1.0 / D) + EPS)
            for b in range(TP):
                v = X[l, b, at_rows, :].astype(F32)
                N[at_rows, pl.ds(b * width, width)] = (v * r * gain[pl.ds(l, 1), pl.ds(b * width, width)]).astype(BF16)
            return 0
        lax.fori_loop(0, GATHER[l][c][1] // step_rows, body, 0)

    def project(l, window):
        first, n = WINDOWS[l][window]
        w = W[l, :, pl.ds(0, depth_in), :].reshape(sps * depth_in, width)
        acc[pl.ds(0, n), :] = jnp.dot(N[pl.ds(first, n), :], w, preferred_element_type=F32)
        for cb in range(width // 128):
            cols = pl.ds(cb * 128, 128)
            p = acc[pl.ds(0, n), cols].astype(BF16).astype(F32)
            s = p
            for i in range(4):
                s = s + jnp.where(masks[i, pl.ds(first, n), :] > 0.5, pltpu.roll(s, 1 << i, 0), 0.0)
            pooled = (s * inv[pl.ds(first, n), :] - p).astype(BF16)
            G[l, half_of, pl.ds(first + 16, n - 16), cols] = pooled[16:, :]

    def mix(l, c):
        first, n = EXCHANGE[l][c]
        a = jnp.zeros((n, width), F32)
        for h in range(2):
            w = W[l, pl.ds(h * (sps // 2), sps // 2), pl.ds(depth_in, depth_mix), :].reshape(sps // 2 * depth_mix, width)
            a = a + jnp.dot(G[l, h, pl.ds(first, n), :], w, preferred_element_type=F32)
        a = a * scale[pl.ds(l, 1), pl.ds(pl.multiple_of(tp * width, width), width)]
        if l == 0:
            X[1, tp, pl.ds(first, n), :] = a.astype(BF16)
        else:
            out[pl.ds(first - HALO, n), :] = a.astype(BF16)

    halo_x = pltpu.make_async_remote_copy(X.at[0, tp, pl.ds(ext - HALO, HALO)], X.at[0, tp, pl.ds(0, HALO)], h_send.at[0], h_recv.at[0], device_id=(nxt, tp), device_id_type=MESH)
    halo_d = pltpu.make_async_remote_copy(docx.at[pl.ds(rows, HALO)], docx.at[pl.ds(0, HALO)], h_send.at[1], h_recv.at[1], device_id=(nxt, tp), device_id_type=MESH)
    halo_x.start()
    halo_d.start()

    def wait(token):
        name = token[0]
        if name == "w":
            layer, which = ROUNDS[token[1]]
            keys = GROUPS[token[1]][GROUP_OF[token[1]][token[2:]]]
            ref = W.at[layer, pl.ds(0, len(keys)), weight_rows[which]]
            if token[4] != "full":
                ref = ref.at[:, :, pl.ds(0, width // 2)]
            pltpu.make_async_copy(ref, ref, w_recv.at[FIRST[token[1]] + GROUP_OF[token[1]][token[2:]]]).wait()
            waited.update(("w", token[1]) + key for key in keys)
        elif name == "x":
            l, who, c = token[1:]
            x_copy(l, who, c, who, tp).wait_recv()
        elif name == "d":
            l, _, c = token[1:]
            ref = X.at[l, pl.ds(0, 4), span(GATHER[l][c])]
            pltpu.make_async_copy(ref, ref, d_recv.at[l, c]).wait()
            waited.update(("d", l, who, c) for who in WHO)
        elif name == "t":
            t_copy(*token[1:], tp).wait_recv()
        elif name == "e":
            l, c = token[1:]
            ref = G.at[l, 1 - half_of, span(EXCHANGE[l][c])]
            pltpu.make_async_remote_copy(ref, ref, e_send.at[l], e_recv.at[l, c], device_id=me, device_id_type=MESH).wait_recv()
        elif name == "halo":
            halo_x.wait_recv()
            halo_d.wait_recv()

    x_way = {1: x_plus, -1: x_minus}
    waited = set()
    ops, _, _ = build()
    for _, op, need in ops:
        for token in need:
            if token not in waited:
                waited.add(token)
                wait(token)
        name = op[0]
        if name == "ws":
            onward(*op[1:])
        elif name == "xs":
            l, who, c, way = op[1:]
            x_copy(l, who, c, {"o": "p" if way == 1 else "m"}.get(who, "2"), x_way[way]).start()
        elif name == "ds":
            d_copy(*op[1:]).start()
        elif name == "es":
            t_copy(*op[1:], x_way[1 if op[2] < 2 else -1]).start()
        elif name == "hl":
            r, dl, dh, way, far = op[1:]
            new = dh - way * far
            half = "full" if abs(new) < 4 else ("A" if way == 1 else "B")
            w_copy(r, dl, dh, half, (dl, 4 if abs(new) == 4 else new, half), at(0, way * far)).start()
        elif name == "ed":
            l, c = op[1:]
            ref = G.at[l, half_of, span(EXCHANGE[l][c])]
            pltpu.make_async_remote_copy(ref, ref, e_send.at[l], e_recv.at[l, c], device_id=(sp, x_two), device_id_type=MESH).start()
        elif name == "ep":
            e_copy(*op[1:], x_way[1 if op[2] < 2 else -1]).start()
        elif name == "norm":
            normalize(op[1], op[2])
        elif name == "project":
            project(op[1], op[2])
        elif name == "mix":
            mix(op[1], op[2])
        elif name == "masks":
            make_masks()

    halo_x.wait_send()
    halo_d.wait_send()
    for r, (layer, which) in enumerate(ROUNDS):
        ref = W.at[layer, pl.ds(0, sps - 1), weight_rows[which]]
        pltpu.make_async_copy(ref, ref, w_send.at[r]).wait()
    for l in range(2):
        ref = X.at[l, pl.ds(0, 7), pl.ds(0, ext - l * HALO // 2)]
        pltpu.make_async_copy(ref, ref, x_send.at[l]).wait()
        ref = G.at[l, pl.ds(0, 1 if l in STRAIGHT else 2), pl.ds(0, ext - (l + 1) * HALO // 2)]
        pltpu.make_async_copy(ref, ref, e_send.at[l]).wait()


def shards(tokens, doc_ids, norm_gain, in_proj, mix_proj, out_scale):
    rows, width = tokens.shape
    depth_in, depth_mix = in_proj.shape[1], mix_proj.shape[1]
    ext = rows + HALO
    docs = doc_ids
    hbm = pl.BlockSpec(memory_space=pl.ANY)
    dma = pltpu.SemaphoreType.DMA
    return pl.pallas_call(
        functools.partial(kernel, rows, width, depth_in, depth_mix),
        name="mixer",
        out_shape=pltpu.VMEM((rows, width), BF16),
        in_specs=[hbm] * 6,
        out_specs=pl.BlockSpec(memory_space=pltpu.VMEM),
        scratch_shapes=[
            pltpu.VMEM((2, RING * RING, depth_in + depth_mix, width), BF16),
            pltpu.VMEM((2, TP, ext, width), BF16),
            pltpu.VMEM((ext, D), BF16),
            pltpu.VMEM((2, 2, ext, width), BF16),
            pltpu.VMEM((2, ext, width), BF16),
            pltpu.VMEM((ext, width), F32),
            pltpu.VMEM((ext, 128), F32),
            pltpu.VMEM((4, ext, 128), F32),
            pltpu.VMEM((ext, 128), F32),
            pltpu.VMEM((rows,), jnp.int32),
            pltpu.VMEM((2, D), F32),
            pltpu.VMEM((2, D), F32),
            dma((8,)),
            dma((len(ROUNDS),)),
            dma((FIRST[-1],)),
            dma((2,)),
            dma((2, 12)),
            dma((2, 4)),
            dma((2,)),
            dma((2, 4)),
            dma((2, 4)),
            dma((2,)),
            dma((2,)),
        ],
        compiler_params=pltpu.CompilerParams(collective_id=0, has_side_effects=True, vmem_limit_bytes=60 * 1024 * 1024),
    )(tokens, docs, norm_gain, in_proj, mix_proj, out_scale)


def solution(mesh):
    placed = (P("sp", "tp"), P("sp"), P(), P(None, "sp", "tp"), P(None, "sp", "tp"), P())
    return jax.shard_map(
        shards, mesh=mesh, in_specs=placed, out_specs=P("sp", "tp"), check_vma=False
    )
```
